32 devices in a mesh: ep: 4 (over y, x), tp: 8 (over z, core).
Axes of the slice: x: 2, y: 2, z: 4, core: 2. Of those that a mesh axis runs over, the one named last changes fastest.
Arguments:
- query_preactivation: bfloat16 [8192, 2048], P('ep', 'tp'), may hold values from -6 to 6
- forget_preactivation: bfloat16 [8192, 2048], P('ep', 'tp'), may hold values from -6 to 6
- value_input_rows: bfloat16 [8192, 1024], P('ep', 'tp'), may hold values from -8 to 8
- output_gate_preactivation: bfloat16 [8192, 1024], P('ep', 'tp'), may hold values from -6 to 6
- forget_floor_gap: float32 [2048], P('tp'), may hold values from 0 to 0.2, as said below
- extra_log_forget: float32 [8192, 16], P('ep', 'tp'), may hold values from -2 to 0
- head_output_gain: float32 [1024], P('tp'), may hold values from 0.1 to 1.9
- mixer_output_weight: bfloat16 [1024, 2048], P(None, 'tp'), may hold values from -0.1875 to 0.1875
- second_batch_tokens: bfloat16 [2048, 2048], P('ep'), may hold values from -6 to 6
- feedforward_norm_gain: float32 [2048], replicated, may hold values from 0.1 to 1.9
- chosen_expert_index: int32 [2048, 2], P('ep'), may hold values from 0 to 3, all different within a row; in each aligned block of 64 rows (0 to 63, 64 to 127, ...) at most 40 rows name the same one
- chosen_expert_weight: float32 [2048, 2], P('ep'), may hold values from 0.1 to 1
- expert_gate_weight: bfloat16 [4, 2048, 7168], P('ep', None, 'tp'), may hold values from -0.125 to 0.125
- expert_up_weight: bfloat16 [4, 2048, 7168], P('ep', None, 'tp'), may hold values from -0.125 to 0.125
- expert_down_weight: bfloat16 [4, 7168, 2048], P('ep', 'tp'), may hold values from -0.0625 to 0.0625
Outputs:
- mixer_output_first: bfloat16 [8192, 2048], P('ep', 'tp')
- moe_out: bfloat16 [2048, 2048], P(('ep', 'tp'))
The draws below stay inside these ranges and needn't reach their ends.
Inputs may be any that keep to these rules, and one draw needn't show every extreme that they name: `chosen_expert_index`: each row names 2 different experts. In each aligned block of 64 rows (the rows of one device's share) no expert is named by more than 40 rows, and in every draw some expert is named by exactly 40 rows of some block. `forget_floor_gap`: every entry is positive.
All inputs are finite; a program needn't handle non-finite values.
Results may differ from the reference program's by a relative error of at most 0.019.
Values may be sent and summed in bfloat16 or wider, within the bound.
No kernel may reach another device: no remote copies, remote signals or barrier semaphores. Data moves between devices by JAX's collectives and lax.ppermute only.
A program may use at most 128 MiB of HBM per device.

```python
import math
import jax
import jax.numpy as jnp
import numpy as np
from jax import lax

D = 2048
RECURRENT_HEADS = 16
KEY_DIM = 128
VAL_DIM = 64
KW = 2048
VW = 1024
BLOCK_POSITIONS = 64
SEG_A = 2048
TOKENS_A = 8192
TOKENS_B = 2048
SUB_B = 64
EXPERTS = 4
FFE = 7168
FFE_DEV = 896
TOPK = 2
CAP = 40
N_TP = 8


def draw_value_input_rows(key, part):
    noise_key, offset_key = jax.random.split(key)
    noise_part = jnp.clip(jax.random.normal(noise_key, (TOKENS_A, VW), jnp.float32), -6.0, 6.0)
    offsets = jax.random.uniform(offset_key, (1, VW), jnp.float32, -1.0, 1.0)
    return (noise_part + offsets).astype(jnp.bfloat16)


def draw_forget_floor_gap(key, part):
    choose_key, slow_key, fast_key = jax.random.split(key, 3)
    slow_share = 0.5
    chosen = jax.random.uniform(choose_key, (KW,), jnp.float32) < slow_share
    slow_rate = jnp.exp(jax.random.uniform(slow_key, (KW,), jnp.float32, jnp.log(0.05 / TOKENS_A), jnp.log(1.0 / TOKENS_A)))
    fast_rate = jnp.exp(jax.random.uniform(fast_key, (KW,), jnp.float32, jnp.log(0.06), jnp.log(0.2)))
    return jnp.where(chosen, slow_rate, fast_rate)


def draw_extra_log_forget(key, part):
    rate_key, place_key, depth_key = jax.random.split(key, 3)
    segments = TOKENS_A // SEG_A
    rates = jnp.exp(jax.random.uniform(rate_key, (segments, 1, RECURRENT_HEADS), jnp.float32, jnp.log(0.1 / TOKENS_A), jnp.log(0.4 / TOKENS_A)))
    base_log = -jnp.broadcast_to(rates, (segments, SEG_A, RECURRENT_HEADS)).reshape(TOKENS_A, RECURRENT_HEADS)
    places = jax.random.randint(place_key, (2, RECURRENT_HEADS), 0, TOKENS_A)
    depths = jax.random.uniform(depth_key, (2, RECURRENT_HEADS), jnp.float32, jnp.log(0.5), jnp.log(0.8))
    columns = jnp.broadcast_to(jnp.arange(RECURRENT_HEADS, dtype=jnp.int32)[None, :], (2, RECURRENT_HEADS))
    return base_log.at[places, columns].add(depths)


def block_scale(own_key, shape, shards, least, high):
    level, own = 1.0, jax.random.fold_in(own_key, 6)
    for axis_at, shards_of in shards:
        heights = jnp.exp(jax.random.uniform(jax.random.fold_in(own, axis_at), (shards_of,), jnp.float32, least / len(shards), high / len(shards)))
        level = level * jnp.repeat(heights, shape[axis_at] // shards_of).reshape([-1 if axis == axis_at else 1 for axis in range(len(shape))])
    return level


def assign_block(own_key, own, number, rows, count, top, limit, lean):
    ranking = jax.random.permutation(own_key, count)
    crowded, usual = portions_of(count, rows * top, limit, lean, True), portions_of(count, rows * top, limit, lean, False)
    places = jnp.arange(count)

    def named(lengths, turn):
        used = int((lengths > 0).sum())
        fixed = max(1, used // 4)
        shifted = fixed + (places - fixed + turn * (used - fixed)) % max(1, count - fixed)
        return jnp.zeros((count,), jnp.int32).at[ranking[jnp.where(places < fixed, places, shifted)]].set(jnp.asarray(lengths, jnp.int32))

    lengths = jnp.where(number % 4 == 0, named(crowded, number // 4), named(usual, number - number // 4 - 1))
    mixed = jax.random.permutation(jax.random.fold_in(own, 3), count)
    giver, receiver = mixed[0:count // 2 * 2:2], mixed[1:count // 2 * 2:2]
    room = jnp.minimum(lengths[giver] - 1, limit - lengths[receiver]) // 2
    room = jnp.where((giver == ranking[0]) | (receiver == ranking[0]) | (lengths[receiver] == 0), 0, jnp.maximum(room, 0))
    shifted = jax.random.randint(jax.random.fold_in(own, 4), (count // 2,), 0, 1 << 20) % (room + 1)
    lengths = lengths.at[giver].add(-shifted).at[receiver].add(shifted)
    labels = jnp.searchsorted(jnp.cumsum(lengths), jnp.arange(rows * top), side="right").astype(jnp.int32)
    listing = labels.reshape(top, rows).T
    listing = listing[jax.random.permutation(jax.random.fold_in(own, 1), rows)]
    turn = jax.random.randint(jax.random.fold_in(own, 2), (rows, 1), 0, top)
    return jnp.take_along_axis(listing, (jnp.arange(top)[None, :] + turn) % top, axis=1)


def portions_of(amount, total, reach, skew, full):
    portions = [(1 << 20) // math.isqrt(grade ** skew) + 1 for grade in range(1, amount + 1)]
    largest = reach if full else min(reach, max(-(-total // amount), total * portions[0] // sum(portions)))
    least = 1 if total - largest >= amount - 1 else 0
    counts, spare = [largest] + [least] * (amount - 1), total - largest - least * (amount - 1)
    while spare > 0:
        candidates = [i for i in range(1, amount) if counts[i] < largest] or [i for i in range(1, amount) if counts[i] < reach]
        pool, left = sum([portions[i] for i in candidates]), spare
        for i in candidates:
            more = min(reach - counts[i], max(1, left * portions[i] // pool), spare)
            counts[i] = counts[i] + more
            spare = spare - more
    return np.array(counts)


def scatter_about(own_key, dims, deviation, bound, cuts=(), kind=jnp.bfloat16):
    array = deviation * jax.random.normal(own_key, dims, jnp.float32)
    if cuts:
        array = array * block_scale(own_key, dims, cuts, -0.22, 0.18)
    return jnp.clip(array, -bound, bound).astype(kind)


def setup_inputs(seed: int = 0) -> dict:
    key_of = jax.random.split(jax.random.key(seed), 16)
    query_preactivation = scatter_about(key_of[0], (TOKENS_A, KW), 1.0, 6.0, ((0, 4), (1, 8)))
    forget_preactivation = scatter_about(key_of[1], (TOKENS_A, KW), 1.0, 6.0, ((0, 4), (1, 8)))
    value_input_rows = draw_value_input_rows(jax.random.fold_in(key_of[15], 71), 0)
    output_gate_preactivation = scatter_about(key_of[3], (TOKENS_A, VW), 1.0, 6.0, ((0, 4), (1, 8)))
    forget_floor_gap = draw_forget_floor_gap(jax.random.fold_in(key_of[15], 71), 0)
    extra_log_forget = draw_extra_log_forget(jax.random.fold_in(key_of[15], 71), 0)
    head_output_gain = jnp.clip(1.0 + 0.18 * jax.random.normal(key_of[6], (VW,), jnp.float32), 0.1, 1.9)
    mixer_output_weight = scatter_about(key_of[7], (VW, D), VW ** -0.5, 0.1875, ((1, 8),))
    second_batch_tokens = scatter_about(key_of[8], (TOKENS_B, D), 1.0, 6.0, ((0, 4),))
    feedforward_norm_gain = jnp.clip(1.0 + 0.18 * jax.random.normal(key_of[9], (D,), jnp.float32), 0.1, 1.9)
    chosen_expert_index_keys = jax.random.split(jax.random.fold_in(key_of[10], 1), TOKENS_B // SUB_B)
    chosen_expert_index_turns = jax.random.permutation(jax.random.fold_in(key_of[10], 3), TOKENS_B // SUB_B)
    chosen_expert_index = jax.vmap(lambda own, number: assign_block(jax.random.fold_in(key_of[10], 2), own, number, SUB_B, EXPERTS, TOPK, CAP, 1))(chosen_expert_index_keys, chosen_expert_index_turns).reshape((TOKENS_B, TOPK))
    chosen_expert_weight = jnp.clip(0.1 + 0.9 * jax.random.uniform(key_of[11], (TOKENS_B, TOPK), jnp.float32) ** block_scale(key_of[11], (TOKENS_B, TOPK), ((0, 4),), -0.2, 0.2), 0.1, 1.0)
    expert_gate_weight = scatter_about(key_of[12], (EXPERTS, D, FFE), D ** -0.5, 0.125, ((0, 4), (2, 8)))
    expert_up_weight = scatter_about(key_of[13], (EXPERTS, D, FFE), D ** -0.5, 0.125, ((0, 4), (2, 8)))
    expert_down_weight = scatter_about(key_of[14], (EXPERTS, FFE, D), FFE ** -0.5, 0.0625, ((0, 4), (1, 8)))
    return {"query_preactivation": query_preactivation, "forget_preactivation": forget_preactivation, "value_input_rows": value_input_rows, "output_gate_preactivation": output_gate_preactivation, "forget_floor_gap": forget_floor_gap, "extra_log_forget": extra_log_forget, "head_output_gain": head_output_gain, "mixer_output_weight": mixer_output_weight, "second_batch_tokens": second_batch_tokens, "feedforward_norm_gain": feedforward_norm_gain, "chosen_expert_index": chosen_expert_index, "chosen_expert_weight": chosen_expert_weight, "expert_gate_weight": expert_gate_weight, "expert_up_weight": expert_up_weight, "expert_down_weight": expert_down_weight}


highest_accuracy = lax.Precision.HIGHEST
epsilon = 1e-06

def slot_positions(blocks):
    flattened = blocks.reshape(blocks.shape[0], -1)
    onehot = (flattened[..., None] == jnp.arange(EXPERTS, dtype=jnp.int32)).astype(jnp.int32)
    earlier = jnp.cumsum(onehot, axis=1) - onehot
    return lax.optimization_barrier(jnp.sum(earlier * onehot, axis=-1)).reshape(blocks.shape)

def mixer_portion(query_preactivation, forget_preactivation, value_input_rows, output_gate_preactivation, forget_floor_gap, extra_log_forget, head_output_gain, mixer_output_weight):
    length = query_preactivation.shape[0]
    block_count = length // BLOCK_POSITIONS
    shape_key = (block_count, BLOCK_POSITIONS, RECURRENT_HEADS, KEY_DIM)
    queries = jax.nn.silu(query_preactivation.astype(jnp.float32)).reshape(shape_key)
    key_decay_rates = forget_floor_gap.reshape(RECURRENT_HEADS, KEY_DIM) * jax.nn.sigmoid(-forget_preactivation.astype(jnp.float32)).reshape(shape_key)
    forget_log_factor = jnp.log(1.0 - key_decay_rates) + extra_log_forget.reshape(block_count, BLOCK_POSITIONS, RECURRENT_HEADS)[..., None]
    values = value_input_rows.astype(jnp.float32).reshape(block_count, BLOCK_POSITIONS, RECURRENT_HEADS, VAL_DIM)
    causal_mask = jnp.arange(BLOCK_POSITIONS)[:, None] >= jnp.arange(BLOCK_POSITIONS)[None, :]

    def advance(recurrent_state_matrix, inputs):
        query_block_rows, block_key, value_block_rows, block_log = inputs
        cumulative_log = jnp.cumsum(block_log, axis=0)
        block_final_row = cumulative_log[-1]
        query_scaled = query_block_rows * jnp.exp(cumulative_log - block_final_row)
        scaled_key_rows = block_key * jnp.exp(block_final_row - cumulative_log)
        scores = jnp.einsum('thk,shk->hts', query_scaled, scaled_key_rows, precision=highest_accuracy)
        scores = jnp.where(causal_mask, scores, 0.0)
        within = jnp.einsum('hts,shv->thv', scores, value_block_rows, precision=highest_accuracy)
        across_blocks = jnp.einsum('pjy,jyr->pjr', query_block_rows * jnp.exp(cumulative_log), recurrent_state_matrix, precision=highest_accuracy)
        recurrent_state_matrix = jnp.exp(block_final_row)[..., None] * recurrent_state_matrix + jnp.einsum('jnz,jne->nze', scaled_key_rows, value_block_rows, precision=highest_accuracy)
        return (recurrent_state_matrix, within + across_blocks)
    initial = jnp.zeros((RECURRENT_HEADS, KEY_DIM, VAL_DIM), jnp.float32)
    final_state, outputs = lax.scan(advance, initial, (queries, key_decay_rates, values, forget_log_factor))
    recurrent = outputs.reshape(length, RECURRENT_HEADS, VAL_DIM)
    factor = lax.rsqrt(lax.optimization_barrier(jnp.mean(recurrent * recurrent, axis=-1, keepdims=True)) + epsilon)
    normed = (recurrent * factor * head_output_gain.reshape(RECURRENT_HEADS, VAL_DIM)).reshape(length, RECURRENT_HEADS * VAL_DIM)
    mixed = (normed * jax.nn.silu(output_gate_preactivation.astype(jnp.float32))).astype(jnp.bfloat16)
    return jnp.dot(mixed, mixer_output_weight, preferred_element_type=jnp.float32).astype(jnp.bfloat16)

def expert_part(second_batch_tokens, feedforward_norm_gain, chosen_expert_index, chosen_expert_weight, expert_gate_weight, expert_up_weight, expert_down_weight):
    total_rows = second_batch_tokens.shape[0]
    width = second_batch_tokens.shape[1]
    tokens_float = second_batch_tokens.astype(jnp.float32)
    factor = lax.rsqrt(lax.optimization_barrier(jnp.mean(tokens_float * tokens_float, axis=-1, keepdims=True)) + epsilon)
    normed = (tokens_float * factor * feedforward_norm_gain).astype(jnp.bfloat16)
    nsub = total_rows // SUB_B
    blocks = chosen_expert_index.reshape(nsub, SUB_B, TOPK)
    slot_ids = slot_positions(blocks)
    sub_index = jnp.arange(nsub, dtype=jnp.int32)[:, None, None]
    flat_slot = (blocks * nsub + sub_index) * CAP + slot_ids
    token_ids = jnp.broadcast_to(jnp.arange(total_rows, dtype=jnp.int32).reshape(nsub, SUB_B, 1), blocks.shape)
    lookup = jnp.full((EXPERTS * nsub * CAP,), -1, jnp.int32).at[flat_slot.reshape(-1)].set(token_ids.reshape(-1))
    lookup = lookup.reshape(EXPERTS, nsub * CAP)

    def one_expert(inputs):
        row_index, gate_weight, up_weight, down_weight = inputs
        picked = normed[jnp.maximum(row_index, 0)]
        routed = jnp.where((row_index >= 0)[:, None], picked, jnp.zeros((), jnp.bfloat16))
        gate_part = jnp.dot(routed, gate_weight, preferred_element_type=jnp.float32)
        up_part = jnp.dot(routed, up_weight, preferred_element_type=jnp.float32)
        hidden = (jax.nn.silu(gate_part) * up_part).astype(jnp.bfloat16)
        hidden_groups = jnp.transpose(hidden.reshape(-1, N_TP, FFE_DEV), (1, 0, 2))
        down_groups = down_weight.reshape(N_TP, FFE_DEV, width)

        def add_group(running, pair):
            product = jnp.dot(pair[0], pair[1], preferred_element_type=jnp.float32)
            return (running + lax.optimization_barrier(product.astype(jnp.bfloat16)).astype(jnp.float32), None)
        running, unused = lax.scan(add_group, jnp.zeros((hidden.shape[0], width), jnp.float32), (hidden_groups, down_groups))
        return running.astype(jnp.bfloat16)
    outputs = lax.map(one_expert, (lookup, expert_gate_weight, expert_up_weight, expert_down_weight))
    flat_outputs = outputs.reshape(-1, width)
    flat_index = flat_slot.reshape(total_rows, TOPK)
    combined = jnp.zeros((total_rows, width), jnp.float32)
    for ranked in range(TOPK):
        combined = combined + flat_outputs[flat_index[:, ranked]].astype(jnp.float32) * chosen_expert_weight[:, ranked:ranked + 1]
    return combined.astype(jnp.bfloat16)

def reference(query_preactivation, forget_preactivation, value_input_rows, output_gate_preactivation, forget_floor_gap, extra_log_forget, head_output_gain, mixer_output_weight, second_batch_tokens, feedforward_norm_gain, chosen_expert_index, chosen_expert_weight, expert_gate_weight, expert_up_weight, expert_down_weight):
    mixer_output_first = mixer_portion(query_preactivation, forget_preactivation, value_input_rows, output_gate_preactivation, forget_floor_gap, extra_log_forget, head_output_gain, mixer_output_weight)
    moe_out = expert_part(second_batch_tokens, feedforward_norm_gain, chosen_expert_index, chosen_expert_weight, expert_gate_weight, expert_up_weight, expert_down_weight)
    return (mixer_output_first, moe_out)
```

```python
import functools
import jax
import jax.numpy as jnp
from jax import lax
from jax.experimental import pallas as pl
from jax.experimental.pallas import tpu as pltpu
from jax.sharding import PartitionSpec as P

KEY_DIM = 128
VAL_DIM = 64
BLOCK = 64
TOPK = 2
CORES = 2
epsilon = 1e-06
f32 = jnp.float32
bf16 = jnp.bfloat16


def mm(a, b, dims=((1,), (0,))):
    return lax.dot_general(a, b, (dims, ((), ())), preferred_element_type=f32)


def split2(x):
    hi = x.astype(bf16)
    return hi, (x - hi.astype(f32)).astype(bf16)


def sigmoid(x):
    return 1.0 / (1.0 + jnp.exp(-x))


def recurrence_body(heads, step_rows, q_ref, f_ref, v_ref, gap_ref, extra_ref, loc_ref, qcd_ref, st_ref, s_ref, l_ref):
    step = pl.program_id(0)
    kw = heads * KEY_DIM
    vw = heads * VAL_DIM
    blocks = step_rows // BLOCK

    @pl.when(step == 0)
    def _():
        s_ref[...] = jnp.zeros_like(s_ref)
        l_ref[...] = jnp.zeros_like(l_ref)

    q = q_ref[...].astype(f32)
    q = q * sigmoid(q)
    key = gap_ref[...] * sigmoid(-f_ref[...].astype(f32))
    extra = extra_ref[...]
    extra = jnp.concatenate(
        [jnp.broadcast_to(extra[:, h : h + 1], (step_rows, KEY_DIM)) for h in range(heads)], axis=1
    )
    logf = jnp.log(1.0 - key) + extra
    row = lax.broadcasted_iota(jnp.int32, (step_rows, step_rows), 0)
    col = lax.broadcasted_iota(jnp.int32, (step_rows, step_rows), 1)
    causal = (row >= col) & (row // BLOCK == col // BLOCK)
    tri = causal.astype(bf16)
    hi, lo = split2(logf)
    cum = mm(tri, hi) + mm(tri, lo)
    v = v_ref[...]
    finals = [cum[(b + 1) * BLOCK - 1 : (b + 1) * BLOCK] for b in range(blocks)]
    fin = jnp.concatenate([jnp.broadcast_to(x, (BLOCK, kw)) for x in finals], axis=0)
    qs = (q * jnp.exp(cum - fin)).astype(bf16)
    ks = (key * jnp.exp(fin - cum)).astype(bf16)
    qc = q * jnp.exp(cum)
    qcb = qc.astype(bf16)
    within = []
    for h in range(heads):
        ksl = slice(h * KEY_DIM, (h + 1) * KEY_DIM)
        sc = mm(qs[:, ksl], ks[:, ksl], ((1,), (1,)))
        sc = jnp.where(causal, sc, 0.0).astype(bf16)
        within.append(mm(sc, v[:, h * VAL_DIM : (h + 1) * VAL_DIM]))
    within = jnp.concatenate(within, axis=1)
    vh = lax.broadcasted_iota(jnp.int32, (vw, kw), 0) // VAL_DIM
    kh = lax.broadcasted_iota(jnp.int32, (vw, kw), 1) // KEY_DIM
    same = vh == kh
    s = s_ref[...]
    l = l_ref[...]
    for b in range(blocks):
        rs = slice(b * BLOCK, (b + 1) * BLOCK)
        loc_ref[rs, :] = within[rs] + mm(qcb[rs], s.astype(bf16), ((1,), (1,)))
        qcd_ref[rs, :] = (qc[rs] * jnp.exp(l)).astype(bf16)
        upd = jnp.where(same, mm(v[rs], ks[rs], ((0,), (0,))), 0.0)
        s = s * jnp.exp(finals[b]) + upd
        l = l + finals[b]
    s_ref[...] = s
    l_ref[...] = l

    @pl.when(step == pl.num_programs(0) - 1)
    def _():
        for h in range(heads):
            st_ref[h * VAL_DIM : (h + 1) * VAL_DIM, :] = s[
                h * VAL_DIM : (h + 1) * VAL_DIM, h * KEY_DIM : (h + 1) * KEY_DIM
            ]
            st_ref[vw + h : vw + h + 1, :] = l[:, h * KEY_DIM : (h + 1) * KEY_DIM]


def recurrence(q, f, v, gap, extra):
    length, kw = q.shape
    heads = kw // KEY_DIM
    vw = heads * VAL_DIM
    rows = 4 * BLOCK
    rows_of = lambda w: pl.BlockSpec((rows, w), lambda i: (i, 0))
    whole = lambda r, w: pl.BlockSpec((r, w), lambda i: (0, 0))
    return pl.pallas_call(
        functools.partial(recurrence_body, heads, rows),
        grid=(length // rows,),
        in_specs=[rows_of(kw), rows_of(kw), rows_of(vw), whole(1, kw), rows_of(heads)],
        out_specs=[rows_of(vw), rows_of(kw), whole(vw + 8, KEY_DIM)],
        out_shape=[
            jax.ShapeDtypeStruct((length, vw), f32),
            jax.ShapeDtypeStruct((length, kw), bf16),
            jax.ShapeDtypeStruct((vw + 8, KEY_DIM), f32),
        ],
        scratch_shapes=[pltpu.VMEM((vw, kw), f32), pltpu.VMEM((1, kw), f32)],
        cost_estimate=pl.CostEstimate(flops=10**10, bytes_accessed=6 * 10**6, transcendentals=10**6),
        name="recurrence",
    )(q, f, v, gap.reshape(1, kw), extra)


def finish_body(heads, ep, me_ref, *refs):
    others = refs[: ep - 1]
    loc_ref, qcd_ref, gate_ref, gain_ref, mixed_ref, c_ref = refs[ep - 1 :]
    kw = heads * KEY_DIM
    vw = heads * VAL_DIM
    me = me_ref[0]

    @pl.when(pl.program_id(0) == 0)
    def _():
        carried = [jnp.zeros((VAL_DIM, KEY_DIM), f32) for _ in range(heads)]
        for j in range(ep):
            use = j < me
            for m in range(1, ep):
                hit = use & ((me ^ m) == j)
                flag = jnp.where(hit, 1.0, 0.0).astype(f32)
                o = others[m - 1]
                for h in range(heads):
                    decay = jnp.exp(o[vw + h : vw + h + 1, :] * flag)
                    carried[h] = carried[h] * decay + o[h * VAL_DIM : (h + 1) * VAL_DIM, :] * flag
        c_ref[...] = jnp.zeros_like(c_ref)
        for h in range(heads):
            c_ref[h * VAL_DIM : (h + 1) * VAL_DIM, h * KEY_DIM : (h + 1) * KEY_DIM] = carried[h].astype(bf16)

    rec = loc_ref[...] + mm(qcd_ref[...], c_ref[...], ((1,), (1,)))
    a = lax.broadcasted_iota(jnp.int32, (vw, vw), 0) // VAL_DIM
    b = lax.broadcasted_iota(jnp.int32, (vw, vw), 1) // VAL_DIM
    ones = (a == b).astype(bf16)
    hi, lo = split2(rec * rec)
    mean = (mm(hi, ones) + mm(lo, ones)) * (1.0 / VAL_DIM)
    g = gate_ref[...].astype(f32)
    mixed_ref[...] = (rec * lax.rsqrt(mean + epsilon) * gain_ref[...] * (g * sigmoid(g))).astype(bf16)


def finish(me, others, loc, qcd, gate, gain):
    length, vw = loc.shape
    kw = qcd.shape[1]
    heads = kw // KEY_DIM
    ep = len(others) + 1
    rows = min(length, 512)
    rows_of = lambda w: pl.BlockSpec((rows, w), lambda i, s: (i, 0))
    whole = lambda r, w: pl.BlockSpec((r, w), lambda i, s: (0, 0))
    return pl.pallas_call(
        functools.partial(finish_body, heads, ep),
        grid_spec=pltpu.PrefetchScalarGridSpec(
            num_scalar_prefetch=1,
            grid=(length // rows,),
            in_specs=[whole(vw + 8, KEY_DIM)] * (ep - 1)
            + [rows_of(vw), rows_of(kw), rows_of(vw), whole(1, vw)],
            out_specs=rows_of(vw),
            scratch_shapes=[pltpu.VMEM((vw, kw), bf16)],
        ),
        out_shape=jax.ShapeDtypeStruct((length, vw), bf16),
        cost_estimate=pl.CostEstimate(flops=3 * 10**9, bytes_accessed=3 * 10**6, transcendentals=10**6),
        name="finish",
    )(me, *others, loc, qcd, gate, gain.reshape(1, vw))


def targets(idx, blk, me, experts, capacity, per_expert):
    n = idx.shape[0]
    lane = lax.broadcasted_iota(jnp.int32, (n, 128), 1)
    picks = [lane == idx[:, r : r + 1] for r in range(TOPK)]
    onehot = jnp.where(picks[0] | picks[1], 1.0, 0.0).astype(bf16)
    row = lax.broadcasted_iota(jnp.int32, (n, n), 0)
    col = lax.broadcasted_iota(jnp.int32, (n, n), 1)
    sub = n // blk[1]
    earlier = ((row > col) & (row // sub == col // sub)).astype(bf16)
    counts = mm(earlier, onehot)
    out = []
    for r in range(TOPK):
        slot = jnp.sum(jnp.where(picks[r], counts, 0.0), axis=1, keepdims=True).astype(jnp.int32)
        out.append((idx[:, r : r + 1] ^ me) * per_expert + blk[0] * capacity + slot)
    return out


def pack_body(experts, capacity, sc_ref, tok_ref, idx_ref, gain_ref, *outs):
    nb, _, sub, width = tok_ref.shape
    n = nb * sub
    x = tok_ref[...].reshape(n, width).astype(f32)
    x = (x * lax.rsqrt(jnp.mean(x * x, axis=1, keepdims=True) + epsilon) * gain_ref[...]).astype(bf16)
    blk = lax.broadcasted_iota(jnp.int32, (n, 1), 0) // sub
    per = nb * capacity
    t = targets(idx_ref[...].reshape(n, TOPK), (blk, nb), sc_ref[0], experts, capacity, per)
    lane = lax.broadcasted_iota(jnp.int32, (n, per), 1)
    for m in range(experts):
        pt = jnp.where((t[0] == lane + m * per) | (t[1] == lane + m * per), 1.0, 0.0).astype(bf16)
        outs[m][...] = mm(pt, x, ((0,), (0,))).astype(bf16)


def pack(scal, tokens, idx, gain, experts, capacity):
    nb, _, sub, width = tokens.shape
    shape = jax.ShapeDtypeStruct((nb * capacity, width), bf16)
    return pl.pallas_call(
        functools.partial(pack_body, experts, capacity),
        grid_spec=pltpu.PrefetchScalarGridSpec(
            num_scalar_prefetch=1,
            grid=(1,),
            in_specs=[
                pl.BlockSpec((nb, 1, sub, width), lambda i, s: (0, s[1], 0, 0)),
                pl.BlockSpec((nb, 1, sub, TOPK), lambda i, s: (0, s[1], 0, 0)),
                pl.BlockSpec((1, width), lambda i, s: (0, 0)),
            ],
            out_specs=[pl.BlockSpec(shape.shape, lambda i, s: (0, 0))] * experts,
        ),
        out_shape=[shape] * experts,
        cost_estimate=pl.CostEstimate(flops=10**9, bytes_accessed=4 * 10**6, transcendentals=10**3),
        name="pack",
    )(scal, tokens, idx, gain.reshape(1, width))


def combine_body(experts, capacity, zn, sc_ref, idx_ref, w_ref, *refs):
    ys = refs[:experts]
    outs = refs[experts:]
    i = pl.program_id(0)
    sub = idx_ref.shape[2]
    blk = sc_ref[2] ^ i
    per = zn * capacity
    t = targets(idx_ref[...].reshape(sub, TOPK), (blk, 1), sc_ref[0], experts, capacity, per)
    w = w_ref[...].reshape(sub, TOPK)
    lane = lax.broadcasted_iota(jnp.int32, (sub, per), 1)
    acc = None
    for m in range(experts):
        c = jnp.where(t[0] == lane + m * per, w[:, 0:1], 0.0) + jnp.where(
            t[1] == lane + m * per, w[:, 1:2], 0.0
        )
        hi, lo = split2(c)
        part = mm(hi, ys[m][...]) + mm(lo, ys[m][...])
        acc = part if acc is None else acc + part
    acc = acc.astype(bf16)
    for m in range(zn):

        @pl.when(i == m)
        def _(m=m):
            outs[m][...] = acc


def combine(scal, idx, w, ys, zn, capacity):
    experts = len(ys)
    sub = idx.shape[2]
    per, width = ys[0].shape
    shape = jax.ShapeDtypeStruct((sub, width), bf16)
    return pl.pallas_call(
        functools.partial(combine_body, experts, capacity, zn),
        grid_spec=pltpu.PrefetchScalarGridSpec(
            num_scalar_prefetch=1,
            grid=(zn,),
            in_specs=[pl.BlockSpec((1, 1, sub, TOPK), lambda i, s: (s[2] ^ i, s[1], 0, 0))] * 2
            + [pl.BlockSpec((per, width), lambda i, s: (0, 0))] * experts,
            out_specs=[pl.BlockSpec((sub, width), lambda i, s: (0, 0))] * zn,
        ),
        out_shape=[shape] * zn,
        cost_estimate=pl.CostEstimate(flops=10**9, bytes_accessed=4 * 10**6, transcendentals=10**3),
        name="combine",
    )(scal, idx, w, *ys)


def on_device(
    query_preactivation,
    forget_preactivation,
    value_input_rows,
    output_gate_preactivation,
    forget_floor_gap,
    extra_log_forget,
    head_output_gain,
    mixer_output_weight,
    second_batch_tokens,
    feedforward_norm_gain,
    chosen_expert_index,
    chosen_expert_weight,
    expert_gate_weight,
    expert_up_weight,
    expert_down_weight,
):
    ep = lax.axis_size("ep")
    tp = lax.axis_size("tp")
    zn = tp // CORES
    me = lax.axis_index("ep").astype(jnp.int32)
    place = lax.axis_index("tp").astype(jnp.int32)
    zi, core = place // CORES, place % CORES
    scal = jnp.stack([me, core, zi])
    over_ep = lambda x, m: lax.ppermute(x, "ep", [(i, i ^ m) for i in range(ep)])
    over_core = lambda x: lax.ppermute(x, "tp", [(i, i ^ 1) for i in range(tp)])
    over_z = lambda x, m: lax.ppermute(x, "tp", [(i, i ^ (m * CORES)) for i in range(tp)])

    assert expert_gate_weight.shape[0] == 1
    experts = ep
    rows, width = second_batch_tokens.shape
    sub = rows // tp
    capacity = max(2, sub * TOPK * 5 // (4 * experts))
    tokens = second_batch_tokens.reshape(zn, CORES, sub, width)
    idx = chosen_expert_index.reshape(zn, CORES, sub, TOPK)
    wts = chosen_expert_weight.reshape(zn, CORES, sub, TOPK)
    packed = pack(scal, tokens, idx, feedforward_norm_gain, experts, capacity)
    arrived = [packed[0]] + [over_ep(packed[m], m) for m in range(1, ep)]
    partner = [over_core(a) for a in arrived]

    loc, qcd, st = recurrence(
        query_preactivation, forget_preactivation, value_input_rows, forget_floor_gap, extra_log_forget
    )
    states = [over_ep(st, m) for m in range(1, ep)]
    mixed = finish(scal, states, loc, qcd, output_gate_preactivation, head_output_gain)
    gathered = [mixed] + [over_z(mixed, m) for m in range(1, zn)]
    swapped = [over_core(g) for g in gathered]
    vw = mixed.shape[1]
    acc = None
    for m in range(zn):
        for x, c in ((gathered[m], core), (swapped[m], 1 - core)):
            wrow = lax.dynamic_slice_in_dim(mixer_output_weight, ((zi ^ m) * CORES + c) * vw, vw, 0)
            part = jnp.dot(x, wrow, preferred_element_type=f32)
            acc = part if acc is None else acc + part
    mixer_output_first = acc.astype(bf16)

    wg, wu, wd = expert_gate_weight[0], expert_up_weight[0], expert_down_weight[0]

    def ffn(x):
        g = jnp.dot(x, wg, preferred_element_type=f32)
        u = jnp.dot(x, wu, preferred_element_type=f32)
        h = (g * jax.nn.sigmoid(g) * u).astype(bf16)
        return jnp.dot(h, wd, preferred_element_type=f32).astype(bf16)

    per = zn * capacity
    y = ffn(jnp.concatenate(partner + arrived, axis=0))
    y_other = y[: ep * per]
    y_own = y[ep * per :]
    from_partner = over_core(y_other)
    pair = y_own.astype(f32) + from_partner.astype(f32)
    sums = [pair[m * per : (m + 1) * per].astype(bf16) for m in range(ep)]
    back = [sums[0]] + [over_ep(sums[m], m) for m in range(1, ep)]
    parts = combine(scal, idx, wts, back, zn, capacity)
    total = parts[0].astype(f32)
    for m in range(1, zn):
        total = total + over_z(parts[m], m).astype(f32)
    return mixer_output_first, total.astype(bf16)


def solution(mesh):
    placed = (
        P("ep", "tp"),
        P("ep", "tp"),
        P("ep", "tp"),
        P("ep", "tp"),
        P("tp"),
        P("ep", "tp"),
        P("tp"),
        P(None, "tp"),
        P("ep", None),
        P(),
        P("ep", None),
        P("ep", None),
        P("ep", None, "tp"),
        P("ep", None, "tp"),
        P("ep", "tp", None),
    )
    return jax.shard_map(
        on_device,
        mesh=mesh,
        in_specs=placed,
        out_specs=(P("ep", "tp"), P(("ep", "tp"), None)),
        check_vma=False,
    )
```

```python
import functools
import jax
import jax.numpy as jnp
from jax import lax
from jax.experimental import pallas as pl
from jax.experimental.pallas import tpu as pltpu
from jax.sharding import PartitionSpec as P


KEY_DIM = 128
VAL_DIM = 64
BLOCK = 64
TOPK = 2
CORES = 2
PIECES = 2
epsilon = 1e-06
f32 = jnp.float32
bf16 = jnp.bfloat16


def mm(a, b, dims=((1,), (0,))):
    return lax.dot_general(a, b, (dims, ((), ())), preferred_element_type=f32)


def split2(x):
    hi = x.astype(bf16)
    return hi, (x - hi.astype(f32)).astype(bf16)


def sigmoid(x):
    return 1.0 / (1.0 + jnp.exp(-x))


def forget_log(heads, f_ref, gap_ref, extra_ref):
    key = gap_ref[...] * sigmoid(-f_ref[...].astype(f32))
    kw = heads * KEY_DIM
    pick = lax.broadcasted_iota(jnp.int32, (heads, kw), 1) // KEY_DIM
    pick = (pick == lax.broadcasted_iota(jnp.int32, (heads, kw), 0)).astype(bf16)
    hi, lo = split2(extra_ref[...])
    extra = mm(hi, pick, ((0,), (0,))) + mm(lo, pick, ((0,), (0,)))
    return key, jnp.log(1.0 - key) + extra


def same_head(heads):
    shape = (heads * VAL_DIM, heads * KEY_DIM)
    vh = lax.broadcasted_iota(jnp.int32, shape, 0) // VAL_DIM
    return vh == lax.broadcasted_iota(jnp.int32, shape, 1) // KEY_DIM


def state_body(heads, rows, f_ref, v_ref, gap_ref, extra_ref, st_ref, s_ref, l_ref):
    step = pl.program_id(0)
    vw = heads * VAL_DIM

    @pl.when(step == 0)
    def _():
        s_ref[...] = jnp.zeros_like(s_ref)
        l_ref[...] = jnp.zeros_like(l_ref)

    key, logf = forget_log(heads, f_ref, gap_ref, extra_ref)
    row = lax.broadcasted_iota(jnp.int32, (rows, rows), 0)
    later = (row < lax.broadcasted_iota(jnp.int32, (rows, rows), 1)).astype(bf16)
    hi, lo = split2(logf)
    rest = mm(later, hi) + mm(later, lo)
    whole = rest[0:1] + logf[0:1]
    ks = (key * jnp.exp(rest)).astype(bf16)
    s = s_ref[...] * jnp.exp(whole) + mm(v_ref[...], ks, ((0,), (0,)))
    l = l_ref[...] + whole
    s_ref[...] = s
    l_ref[...] = l

    @pl.when(step == pl.num_programs(0) - 1)
    def _():
        for h in range(heads):
            st_ref[h * VAL_DIM : (h + 1) * VAL_DIM, :] = s[
                h * VAL_DIM : (h + 1) * VAL_DIM, h * KEY_DIM : (h + 1) * KEY_DIM
            ]
            st_ref[vw + h : vw + h + 1, :] = l[:, h * KEY_DIM : (h + 1) * KEY_DIM]


def final_state(f, v, gap, extra):
    length, kw = f.shape
    heads = kw // KEY_DIM
    vw = heads * VAL_DIM
    rows = 4 * BLOCK
    rows_of = lambda w: pl.BlockSpec((rows, w), lambda i: (i, 0))
    whole = lambda r, w: pl.BlockSpec((r, w), lambda i: (0, 0))
    return pl.pallas_call(
        functools.partial(state_body, heads, rows),
        grid=(length // rows,),
        in_specs=[rows_of(kw), rows_of(vw), whole(1, kw), pl.BlockSpec((heads, rows), lambda i: (0, i))],
        out_specs=whole(vw + 8, KEY_DIM),
        out_shape=jax.ShapeDtypeStruct((vw + 8, KEY_DIM), f32),
        scratch_shapes=[pltpu.VMEM((vw, kw), f32), pltpu.VMEM((1, kw), f32)],
        cost_estimate=pl.CostEstimate(flops=4 * 10**9, bytes_accessed=2 * 10**6, transcendentals=10**6),
        name="final_state",
    )(f, v, gap.reshape(1, kw), extra)


def mixer_body(heads, ep, rows, sc_ref, *refs):
    others = refs[: ep - 1]
    q_ref, f_ref, v_ref, gate_ref, gap_ref, extra_ref, gain_ref, mixed_ref, s_ref = refs[ep - 1 :]
    kw = heads * KEY_DIM
    vw = heads * VAL_DIM
    blocks = rows // BLOCK
    me = sc_ref[0]

    @pl.when(pl.program_id(0) == 0)
    def _():
        carried = [jnp.zeros((VAL_DIM, KEY_DIM), f32) for _ in range(heads)]
        for j in range(ep):
            use = j < me
            for m in range(1, ep):
                flag = jnp.where(use & ((me ^ m) == j), 1.0, 0.0).astype(f32)
                o = others[m - 1]
                for h in range(heads):
                    decay = jnp.exp(o[vw + h : vw + h + 1, :] * flag)
                    carried[h] = carried[h] * decay + o[h * VAL_DIM : (h + 1) * VAL_DIM, :] * flag
        s_ref[...] = jnp.zeros_like(s_ref)
        for h in range(heads):
            s_ref[h * VAL_DIM : (h + 1) * VAL_DIM, h * KEY_DIM : (h + 1) * KEY_DIM] = carried[h]

    q = q_ref[...].astype(f32)
    q = q * sigmoid(q)
    key, logf = forget_log(heads, f_ref, gap_ref, extra_ref)
    row = lax.broadcasted_iota(jnp.int32, (rows, rows), 0)
    col = lax.broadcasted_iota(jnp.int32, (rows, rows), 1)
    causal = (row >= col) & (row // BLOCK == col // BLOCK)
    tri = causal.astype(bf16)
    hi, lo = split2(logf)
    cum = mm(tri, hi) + mm(tri, lo)
    v = v_ref[...]
    finals = [cum[(b + 1) * BLOCK - 1 : (b + 1) * BLOCK] for b in range(blocks)]
    fin = jnp.concatenate([jnp.broadcast_to(x, (BLOCK, kw)) for x in finals], axis=0)
    qs = (q * jnp.exp(cum - fin)).astype(bf16)
    ks = (key * jnp.exp(fin - cum)).astype(bf16)
    qc = (q * jnp.exp(cum)).astype(bf16)
    within = []
    for h in range(heads):
        ksl = slice(h * KEY_DIM, (h + 1) * KEY_DIM)
        sc = mm(qs[:, ksl], ks[:, ksl], ((1,), (1,)))
        sc = jnp.where(causal, sc, 0.0).astype(bf16)
        within.append(mm(sc, v[:, h * VAL_DIM : (h + 1) * VAL_DIM]))
    within = jnp.concatenate(within, axis=1)
    same = same_head(heads)
    s = s_ref[...]
    across = []
    for b in range(blocks):
        rs = slice(b * BLOCK, (b + 1) * BLOCK)
        across.append(mm(qc[rs], s.astype(bf16), ((1,), (1,))))
        upd = jnp.where(same, mm(v[rs], ks[rs], ((0,), (0,))), 0.0)
        s = s * jnp.exp(finals[b]) + upd
    s_ref[...] = s
    rec = within + jnp.concatenate(across, axis=0)
    a = lax.broadcasted_iota(jnp.int32, (vw, vw), 0) // VAL_DIM
    b = lax.broadcasted_iota(jnp.int32, (vw, vw), 1) // VAL_DIM
    ones = (a == b).astype(bf16)
    hi, lo = split2(rec * rec)
    mean = (mm(hi, ones) + mm(lo, ones)) * (1.0 / VAL_DIM)
    g = gate_ref[...].astype(f32)
    mixed_ref[...] = (rec * lax.rsqrt(mean + epsilon) * gain_ref[...] * (g * sigmoid(g))).astype(bf16)


def mixer(scal, others, q, f, v, gate, gap, extra, gain):
    length, kw = q.shape
    heads = kw // KEY_DIM
    vw = heads * VAL_DIM
    ep = len(others) + 1
    rows = 4 * BLOCK
    rows_of = lambda w: pl.BlockSpec((rows, w), lambda i, s: (i, 0))
    whole = lambda r, w: pl.BlockSpec((r, w), lambda i, s: (0, 0))
    return pl.pallas_call(
        functools.partial(mixer_body, heads, ep, rows),
        grid_spec=pltpu.PrefetchScalarGridSpec(
            num_scalar_prefetch=1,
            grid=(length // rows,),
            in_specs=[whole(vw + 8, KEY_DIM)] * (ep - 1)
            + [rows_of(kw), rows_of(kw), rows_of(vw), rows_of(vw), whole(1, kw)]
            + [pl.BlockSpec((heads, rows), lambda i, s: (0, i)), whole(1, vw)],
            out_specs=rows_of(vw),
            scratch_shapes=[pltpu.VMEM((vw, kw), f32)],
        ),
        out_shape=jax.ShapeDtypeStruct((length, vw), bf16),
        cost_estimate=pl.CostEstimate(flops=12 * 10**9, bytes_accessed=4 * 10**6, transcendentals=10**6),
        name="mixer",
    )(scal, *others, q, f, v, gate, gap.reshape(1, kw), extra, gain.reshape(1, vw))


def project_body(zn, sc_ref, *refs):
    gs = refs[:zn]
    w_ref, wp_ref, own_ref, other_ref = refs[zn:]
    vw = gs[0].shape[1]
    own = other = None
    for m in range(zn):
        at = pl.multiple_of(((sc_ref[2] ^ m) * CORES + sc_ref[1]) * vw, vw)
        g = gs[m][...]
        a = mm(g, w_ref[pl.ds(at, vw), :])
        b = mm(g, wp_ref[pl.ds(at, vw), :])
        own = a if own is None else own + a
        other = b if other is None else other + b
    own_ref[...] = own
    other_ref[...] = other.astype(bf16)


def project(scal, gathered, w, wp):
    length, vw = gathered[0].shape
    zn = len(gathered)
    rows = min(length, 512)
    rows_of = lambda n: pl.BlockSpec((rows, n), lambda i, s: (i, 0))
    whole = pl.BlockSpec(w.shape, lambda i, s: (0, 0))
    width = w.shape[1]
    return pl.pallas_call(
        functools.partial(project_body, zn),
        grid_spec=pltpu.PrefetchScalarGridSpec(
            num_scalar_prefetch=1,
            grid=(length // rows,),
            in_specs=[rows_of(vw)] * zn + [whole, whole],
            out_specs=[rows_of(width), rows_of(width)],
        ),
        out_shape=[
            jax.ShapeDtypeStruct((length, width), f32),
            jax.ShapeDtypeStruct((length, width), bf16),
        ],
        cost_estimate=pl.CostEstimate(flops=2 * 10**9, bytes_accessed=6 * 10**6, transcendentals=0),
        name="project",
    )(scal, *gathered, w, wp)


def own_lanes(x, zn, sub, core):
    out = None
    for c in range(CORES):
        at = [(z * CORES + c) * sub for z in range(zn)]
        part = jnp.concatenate([x[:, a : a + sub] for a in at], axis=1)
        out = part if out is None else jnp.where(core == c, part, out)
    return out


def targets(idx, me, zn, experts, capacity):
    n = idx.shape[1]
    sub = n // zn
    lines = max(8, experts)
    line = lax.broadcasted_iota(jnp.int32, (lines, n), 0)
    picks = [line == idx[r : r + 1] for r in range(TOPK)]
    onehot = jnp.where(picks[0] | picks[1], 1.0, 0.0).astype(bf16)
    row = lax.broadcasted_iota(jnp.int32, (n, n), 0)
    col = lax.broadcasted_iota(jnp.int32, (n, n), 1)
    earlier = ((row < col) & (row // sub == col // sub)).astype(bf16)
    counts = mm(onehot, earlier)
    blk = lax.broadcasted_iota(jnp.int32, (1, n), 1) // sub
    out = []
    for r in range(TOPK):
        slot = jnp.sum(jnp.where(picks[r], counts, 0.0), axis=0, keepdims=True).astype(jnp.int32)
        out.append((idx[r : r + 1] ^ me) * (zn * capacity) + blk * capacity + slot)
    return out


def pack_body(experts, capacity, sc_ref, tok_ref, idx_ref, gain_ref, *outs):
    zn, _, sub, width = tok_ref.shape
    n = zn * sub
    x = tok_ref[...].reshape(n, width).astype(f32)
    x = (x * lax.rsqrt(jnp.mean(x * x, axis=1, keepdims=True) + epsilon) * gain_ref[...]).astype(bf16)
    t = targets(own_lanes(idx_ref[...], zn, sub, sc_ref[1]), sc_ref[0], zn, experts, capacity)
    per = zn * capacity
    line = lax.broadcasted_iota(jnp.int32, (per, n), 0)
    for m in range(experts):
        hit = (t[0] == line + m * per) | (t[1] == line + m * per)
        outs[m][...] = mm(jnp.where(hit, 1.0, 0.0).astype(bf16), x).astype(bf16)


def pack(scal, tokens, idx, gain, experts, capacity):
    zn, _, sub, width = tokens.shape
    shape = jax.ShapeDtypeStruct((zn * capacity, width), bf16)
    return pl.pallas_call(
        functools.partial(pack_body, experts, capacity),
        grid_spec=pltpu.PrefetchScalarGridSpec(
            num_scalar_prefetch=1,
            grid=(1,),
            in_specs=[
                pl.BlockSpec((zn, 1, sub, width), lambda i, s: (0, s[1], 0, 0)),
                pl.BlockSpec(idx.shape, lambda i, s: (0, 0)),
                pl.BlockSpec((1, width), lambda i, s: (0, 0)),
            ],
            out_specs=[pl.BlockSpec(shape.shape, lambda i, s: (0, 0))] * experts,
        ),
        out_shape=[shape] * experts,
        cost_estimate=pl.CostEstimate(flops=4 * 10**9, bytes_accessed=4 * 10**6, transcendentals=10**3),
        name="pack",
    )(scal, tokens, idx, gain.reshape(1, width))


def ffn_body(count, pieces, *refs):
    xs = refs[:count]
    wg, wgp, wu, wup, wd, wdp = refs[count : count + 6]
    outs = refs[count + 6 : -2]
    x_ref, acc_ref = refs[-2:]
    step = pl.program_id(0)
    per = xs[0].shape[0]

    @pl.when(step == 0)
    def _():
        x_ref[...] = jnp.concatenate([x[...] for x in xs], axis=0)
        acc_ref[...] = jnp.zeros_like(acc_ref)

    x = x_ref[...]
    g = mm(x, jnp.concatenate([wg[0], wgp[0]], axis=1))
    u = mm(x, jnp.concatenate([wu[0], wup[0]], axis=1))
    h = (g * sigmoid(g) * u).astype(bf16)
    acc_ref[...] += mm(h, jnp.concatenate([wd[0], wdp[0]], axis=0))

    @pl.when(step == pl.num_programs(0) - 1)
    def _():
        cols = x_ref.shape[1] // pieces
        for i in range(count):
            for p in range(pieces):
                outs[i * pieces + p][...] = acc_ref[
                    i * per : (i + 1) * per, p * cols : (p + 1) * cols
                ].astype(bf16)


def ffn(xs, weights, pieces):
    count = len(xs)
    per, width = xs[0].shape
    hidden = weights[0].shape[2]
    chunk = 128 if hidden % 128 == 0 else hidden
    whole = pl.BlockSpec((per, width), lambda i: (0, 0))
    out = pl.BlockSpec((per, width // pieces), lambda i: (0, 0))
    up = pl.BlockSpec((1, width, chunk), lambda i: (0, 0, i))
    down = pl.BlockSpec((1, chunk, width), lambda i: (0, i, 0))
    outs = pl.pallas_call(
        functools.partial(ffn_body, count, pieces),
        grid=(hidden // chunk,),
        in_specs=[whole] * count + [up] * 4 + [down] * 2,
        out_specs=[out] * (count * pieces),
        out_shape=[jax.ShapeDtypeStruct((per, width // pieces), bf16)] * (count * pieces),
        scratch_shapes=[pltpu.VMEM((count * per, width), bf16), pltpu.VMEM((count * per, width), f32)],
        cost_estimate=pl.CostEstimate(flops=8 * 10**9, bytes_accessed=25 * 10**6, transcendentals=10**6),
        name="ffn",
    )(*xs, *weights)
    return [outs[i * pieces : (i + 1) * pieces] for i in range(count)]


def combine_body(experts, capacity, zn, sc_ref, idx_ref, w_ref, *refs):
    ys = refs[:experts]
    outs = refs[experts : experts + zn]
    acc_ref = refs[-1]
    sub = outs[0].shape[0]
    n = zn * sub
    t = targets(own_lanes(idx_ref[...], zn, sub, sc_ref[1]), sc_ref[0], zn, experts, capacity)
    w = own_lanes(w_ref[...], zn, sub, sc_ref[1])
    per = zn * capacity
    line = lax.broadcasted_iota(jnp.int32, (per, n), 0)
    acc = None
    for m in range(experts):
        c = jnp.where(t[0] == line + m * per, w[0:1], 0.0)
        c = c + jnp.where(t[1] == line + m * per, w[1:2], 0.0)
        part = mm(c.astype(bf16), ys[m][...], ((0,), (0,)))
        acc = part if acc is None else acc + part
    acc_ref[...] = acc.reshape(zn, sub, acc.shape[1]).astype(bf16)
    for m in range(zn):
        outs[m][...] = acc_ref[sc_ref[2] ^ m]


def combine(scal, idx, w, ys, piece, pieces, zn, sub, capacity):
    experts = len(ys)
    per = zn * capacity
    cols = ys[0].shape[1] // pieces if ys[0].shape[1] == max(y.shape[1] for y in ys) else ys[0].shape[1]
    shape = jax.ShapeDtypeStruct((sub, cols), bf16)
    return pl.pallas_call(
        functools.partial(combine_body, experts, capacity, zn),
        grid_spec=pltpu.PrefetchScalarGridSpec(
            num_scalar_prefetch=1,
            grid=(1,),
            in_specs=[pl.BlockSpec(idx.shape, lambda i, s: (0, 0))] * 2
            + [
                pl.BlockSpec((per, cols), (lambda i, s: (0, piece)) if y.shape[1] != cols else (lambda i, s: (0, 0)))
                for y in ys
            ],
            out_specs=[pl.BlockSpec(shape.shape, lambda i, s: (0, 0))] * zn,
            scratch_shapes=[pltpu.VMEM((zn, sub, cols), bf16)],
        ),
        out_shape=[shape] * zn,
        cost_estimate=pl.CostEstimate(flops=10**9, bytes_accessed=2 * 10**6, transcendentals=10**3),
        name="combine",
    )(scal, idx, w, *ys)


def on_device(
    query_preactivation,
    forget_preactivation,
    value_input_rows,
    output_gate_preactivation,
    forget_floor_gap,
    extra_log_forget,
    head_output_gain,
    mixer_output_weight,
    second_batch_tokens,
    feedforward_norm_gain,
    chosen_expert_index,
    chosen_expert_weight,
    expert_gate_weight,
    expert_up_weight,
    expert_down_weight,
):
    ep = lax.axis_size("ep")
    tp = lax.axis_size("tp")
    zn = tp // CORES
    me = lax.axis_index("ep").astype(jnp.int32)
    place = lax.axis_index("tp").astype(jnp.int32)
    zi, core = place >> 1, place & 1
    scal = jnp.stack([me, core, zi])
    over_ep = lambda x, m: lax.ppermute(x, "ep", [(i, i ^ m) for i in range(ep)])
    over_core = lambda x: lax.ppermute(x, "tp", [(i, i ^ 1) for i in range(tp)])
    over_z = lambda x, m: lax.ppermute(x, "tp", [(i, i ^ (m * CORES)) for i in range(tp)])
    tie = lax.optimization_barrier
    assert expert_gate_weight.shape[0] == 1
    experts = ep
    rows, width = second_batch_tokens.shape
    sub = rows // tp
    capacity = max(2, sub * TOPK * 5 // (4 * experts))
    pieces = PIECES
    extra = extra_log_forget.T
    idx = chosen_expert_index.T
    wts = chosen_expert_weight.T

    weights = []
    for w in (expert_gate_weight, expert_up_weight, expert_down_weight):
        weights += [w, over_core(w)]
    wp = over_core(mixer_output_weight)

    st = final_state(forget_preactivation, value_input_rows, forget_floor_gap, extra)
    states = [over_ep(st, m) for m in range(1, ep)]

    tokens, _ = tie((second_batch_tokens, st))
    tokens = tokens.reshape(zn, CORES, sub, width)
    packed = pack(scal, tokens, idx, feedforward_norm_gain, experts, capacity)
    order = [ep - 1] + list(range(1, ep - 1))
    arrived = {0: packed[0]}
    for m in order:
        arrived[m] = over_ep(packed[m], m)

    q, _ = tie((query_preactivation, packed[1]))
    mixed = mixer(
        scal,
        states,
        q,
        forget_preactivation,
        value_input_rows,
        output_gate_preactivation,
        forget_floor_gap,
        extra,
        head_output_gain,
    )
    gathered = [mixed]
    for m in range(1, zn):
        chained = m % 2 == 1 and m > 1
        gathered.append(over_z(gathered[m - 1] if chained else mixed, 1 if chained else m))

    x0, _ = tie((arrived[0], mixed))
    (y1,), (y0,) = ffn([arrived[ep - 1], x0], weights, 1)
    late = ffn([arrived[m] for m in order[1:]], weights, pieces)
    first_back = over_ep(y1, ep - 1)
    back = [[over_ep(late[i][p], m) for i, m in enumerate(order[1:])] for p in range(pieces)]
    own, other = project(scal, gathered, mixer_output_weight, wp)
    other = over_core(other)
    mixer_output_first = (own + other.astype(f32)).astype(bf16)
    outs = []
    for p in range(pieces):
        ys = [y0] + back[p] + [first_back]
        parts = combine(scal, idx, wts, ys, p, pieces, zn, sub, capacity)
        total = parts[0].astype(f32)
        for m in range(1, zn):
            total = total + over_z(parts[m], m).astype(f32)
        outs.append(total.astype(bf16))
    return mixer_output_first, jnp.concatenate(outs, axis=1)


def solution(mesh):
    placed = (
        P("ep", "tp"),
        P("ep", "tp"),
        P("ep", "tp"),
        P("ep", "tp"),
        P("tp"),
        P("ep", "tp"),
        P("tp"),
        P(None, "tp"),
        P("ep", None),
        P(),
        P("ep", None),
        P("ep", None),
        P("ep", None, "tp"),
        P("ep", None, "tp"),
        P("ep", "tp", None),
    )

    return jax.shard_map(
        on_device,
        mesh=mesh,
        in_specs=placed,
        out_specs=(P("ep", "tp"), P(("ep", "tp"), None)),
        check_vma=False,
    )
```

```python
import functools
import jax
import jax.numpy as jnp
from jax import lax
from jax.experimental import pallas as pl
from jax.experimental.pallas import tpu as pltpu
from jax.sharding import PartitionSpec as P


KEY_DIM = 128
VAL_DIM = 64
BLOCK = 64
TOPK = 2
CORES = 2
PIECES = 2
STATE_ROWS = 2048
MIXER_ROWS = 2048
FFN_VMEM = 36 * 1024 * 1024
VMEM = 20 * 1024 * 1024
epsilon = 1e-06
f32 = jnp.float32
bf16 = jnp.bfloat16


def mm(a, b, dims=((1,), (0,))):
    return lax.dot_general(a, b, (dims, ((), ())), preferred_element_type=f32)


def split2(x):
    hi = x.astype(bf16)
    return hi, (x - hi.astype(f32)).astype(bf16)


def sigmoid(x):
    return 0.5 + 0.5 * jnp.tanh(0.5 * x)


def forget_log(heads, f, gap, extra):
    key = gap * sigmoid(-f.astype(f32))
    kw = heads * KEY_DIM
    pick = lax.broadcasted_iota(jnp.int32, (heads, kw), 1) // KEY_DIM
    pick = (pick == lax.broadcasted_iota(jnp.int32, (heads, kw), 0)).astype(bf16)
    hi, lo = split2(extra)
    extra = mm(hi, pick, ((0,), (0,))) + mm(lo, pick, ((0,), (0,)))
    return key, jnp.log(1.0 - key) + extra


def same_head(heads):
    shape = (heads * VAL_DIM, heads * KEY_DIM)
    vh = lax.broadcasted_iota(jnp.int32, shape, 0) // VAL_DIM
    return vh == lax.broadcasted_iota(jnp.int32, shape, 1) // KEY_DIM


def state_body(heads, rows, f_ref, v_ref, gap_ref, extra_ref, st_ref, s_ref, l_ref):
    step = pl.program_id(0)
    vw = heads * VAL_DIM

    @pl.when(step == 0)
    def _():
        s_ref[...] = jnp.zeros_like(s_ref)
        l_ref[...] = jnp.zeros_like(l_ref)

    row = lax.broadcasted_iota(jnp.int32, (rows, rows), 0)
    later = (row < lax.broadcasted_iota(jnp.int32, (rows, rows), 1)).astype(bf16)
    s = s_ref[...]
    l = l_ref[...]
    for at in range(0, f_ref.shape[0], rows):
        rs = slice(at, at + rows)
        key, logf = forget_log(heads, f_ref[rs, :], gap_ref[...], extra_ref[:, rs])
        hi, lo = split2(logf)
        rest = mm(later, hi) + mm(later, lo)
        whole = rest[0:1] + logf[0:1]
        ks = (key * jnp.exp(rest)).astype(bf16)
        s = s * jnp.exp(whole) + mm(v_ref[rs, :], ks, ((0,), (0,)))
        l = l + whole
    s_ref[...] = s
    l_ref[...] = l

    @pl.when(step == pl.num_programs(0) - 1)
    def _():
        for h in range(heads):
            st_ref[h * VAL_DIM : (h + 1) * VAL_DIM, :] = s[
                h * VAL_DIM : (h + 1) * VAL_DIM, h * KEY_DIM : (h + 1) * KEY_DIM
            ]
            st_ref[vw + h : vw + h + 1, :] = l[:, h * KEY_DIM : (h + 1) * KEY_DIM]


def final_state(f, v, gap, extra):
    length, kw = f.shape
    heads = kw // KEY_DIM
    vw = heads * VAL_DIM
    rows = min(length, STATE_ROWS)
    rows_of = lambda w: pl.BlockSpec((rows, w), lambda i: (i, 0))
    whole = lambda r, w: pl.BlockSpec((r, w), lambda i: (0, 0))
    return pl.pallas_call(
        functools.partial(state_body, heads, 4 * BLOCK),
        grid=(length // rows,),
        in_specs=[rows_of(kw), rows_of(vw), whole(1, kw), pl.BlockSpec((heads, rows), lambda i: (0, i))],
        out_specs=whole(vw + 8, KEY_DIM),
        out_shape=jax.ShapeDtypeStruct((vw + 8, KEY_DIM), f32),
        scratch_shapes=[pltpu.VMEM((vw, kw), f32), pltpu.VMEM((1, kw), f32)],
        cost_estimate=pl.CostEstimate(flops=4 * 10**9, bytes_accessed=2 * 10**6, transcendentals=10**6),
        compiler_params=pltpu.CompilerParams(vmem_limit_bytes=VMEM),
        name="final_state",
    )(f, v, gap.reshape(1, kw), extra)


def mixer_body(heads, ep, rows, sc_ref, *refs):
    others = refs[: ep - 1]
    q_ref, f_ref, v_ref, gate_ref, gap_ref, extra_ref, gain_ref, mixed_ref, s_ref = refs[ep - 1 :]
    kw = heads * KEY_DIM
    vw = heads * VAL_DIM
    blocks = rows // BLOCK
    me = sc_ref[0]

    @pl.when(pl.program_id(0) == 0)
    def _():
        carried = [jnp.zeros((VAL_DIM, KEY_DIM), f32) for _ in range(heads)]
        for j in range(ep):
            use = j < me
            for m in range(1, ep):
                flag = jnp.where(use & ((me ^ m) == j), 1.0, 0.0).astype(f32)
                o = others[m - 1]
                for h in range(heads):
                    decay = jnp.exp(o[vw + h : vw + h + 1, :] * flag)
                    carried[h] = carried[h] * decay + o[h * VAL_DIM : (h + 1) * VAL_DIM, :] * flag
        s_ref[...] = jnp.zeros_like(s_ref)
        for h in range(heads):
            s_ref[h * VAL_DIM : (h + 1) * VAL_DIM, h * KEY_DIM : (h + 1) * KEY_DIM] = carried[h]

    row = lax.broadcasted_iota(jnp.int32, (rows, rows), 0)
    col = lax.broadcasted_iota(jnp.int32, (rows, rows), 1)
    causal = (row >= col) & (row // BLOCK == col // BLOCK)
    tri = causal.astype(bf16)
    same = same_head(heads)
    a = lax.broadcasted_iota(jnp.int32, (vw, vw), 0) // VAL_DIM
    b = lax.broadcasted_iota(jnp.int32, (vw, vw), 1) // VAL_DIM
    ones = (a == b).astype(bf16)
    s = s_ref[...]
    for at in range(0, q_ref.shape[0], rows):
        part = slice(at, at + rows)
        q = q_ref[part, :].astype(f32)
        q = q * sigmoid(q)
        key, logf = forget_log(heads, f_ref[part, :], gap_ref[...], extra_ref[:, part])
        hi, lo = split2(logf)
        cum = mm(tri, hi) + mm(tri, lo)
        v = v_ref[part, :]
        finals = [cum[(b + 1) * BLOCK - 1 : (b + 1) * BLOCK] for b in range(blocks)]
        fin = jnp.concatenate([jnp.broadcast_to(x, (BLOCK, kw)) for x in finals], axis=0)
        qs = (q * jnp.exp(cum - fin)).astype(bf16)
        ks = (key * jnp.exp(fin - cum)).astype(bf16)
        qc = (q * jnp.exp(cum)).astype(bf16)
        within = []
        for h in range(heads):
            ksl = slice(h * KEY_DIM, (h + 1) * KEY_DIM)
            sc = mm(qs[:, ksl], ks[:, ksl], ((1,), (1,)))
            sc = jnp.where(causal, sc, 0.0).astype(bf16)
            within.append(mm(sc, v[:, h * VAL_DIM : (h + 1) * VAL_DIM]))
        within = jnp.concatenate(within, axis=1)
        across = []
        for b in range(blocks):
            rs = slice(b * BLOCK, (b + 1) * BLOCK)
            across.append(mm(qc[rs], s.astype(bf16), ((1,), (1,))))
            upd = jnp.where(same, mm(v[rs], ks[rs], ((0,), (0,))), 0.0)
            s = s * jnp.exp(finals[b]) + upd
        rec = within + jnp.concatenate(across, axis=0)
        hi, lo = split2(rec * rec)
        mean = (mm(hi, ones) + mm(lo, ones)) * (1.0 / VAL_DIM)
        g = gate_ref[part, :].astype(f32)
        mixed_ref[part, :] = (
            rec * lax.rsqrt(mean + epsilon) * gain_ref[...] * (g * sigmoid(g))
        ).astype(bf16)
    s_ref[...] = s


def mixer(scal, others, q, f, v, gate, gap, extra, gain):
    length, kw = q.shape
    heads = kw // KEY_DIM
    vw = heads * VAL_DIM
    ep = len(others) + 1
    rows = min(length, MIXER_ROWS)
    rows_of = lambda w: pl.BlockSpec((rows, w), lambda i, s: (i, 0))
    whole = lambda r, w: pl.BlockSpec((r, w), lambda i, s: (0, 0))
    return pl.pallas_call(
        functools.partial(mixer_body, heads, ep, 4 * BLOCK),
        grid_spec=pltpu.PrefetchScalarGridSpec(
            num_scalar_prefetch=1,
            grid=(length // rows,),
            in_specs=[whole(vw + 8, KEY_DIM)] * (ep - 1)
            + [rows_of(kw), rows_of(kw), rows_of(vw), rows_of(vw), whole(1, kw)]
            + [pl.BlockSpec((heads, rows), lambda i, s: (0, i)), whole(1, vw)],
            out_specs=rows_of(vw),
            scratch_shapes=[pltpu.VMEM((vw, kw), f32)],
        ),
        out_shape=jax.ShapeDtypeStruct((length, vw), bf16),
        cost_estimate=pl.CostEstimate(flops=12 * 10**9, bytes_accessed=4 * 10**6, transcendentals=10**6),
        compiler_params=pltpu.CompilerParams(vmem_limit_bytes=VMEM),
        name="mixer",
    )(scal, *others, q, f, v, gate, gap.reshape(1, kw), extra, gain.reshape(1, vw))


def project_body(zn, sc_ref, *refs):
    gs = refs[:zn]
    w_ref, wp_ref, own_ref, other_ref = refs[zn:]
    vw = gs[0].shape[1]
    own = other = None
    for m in range(zn):
        at = pl.multiple_of(((sc_ref[2] ^ m) * CORES + sc_ref[1]) * vw, vw)
        g = gs[m][...]
        a = mm(g, w_ref[pl.ds(at, vw), :])
        b = mm(g, wp_ref[pl.ds(at, vw), :])
        own = a if own is None else own + a
        other = b if other is None else other + b
    own_ref[...] = own
    other_ref[...] = other.astype(bf16)


def project(scal, gathered, w, wp):
    length, vw = gathered[0].shape
    zn = len(gathered)
    rows = min(length, 1024)
    rows_of = lambda n: pl.BlockSpec((rows, n), lambda i, s: (i, 0))
    whole = pl.BlockSpec(w.shape, lambda i, s: (0, 0))
    width = w.shape[1]
    return pl.pallas_call(
        functools.partial(project_body, zn),
        grid_spec=pltpu.PrefetchScalarGridSpec(
            num_scalar_prefetch=1,
            grid=(length // rows,),
            in_specs=[rows_of(vw)] * zn + [whole, whole],
            out_specs=[rows_of(width), rows_of(width)],
        ),
        out_shape=[
            jax.ShapeDtypeStruct((length, width), f32),
            jax.ShapeDtypeStruct((length, width), bf16),
        ],
        cost_estimate=pl.CostEstimate(flops=2 * 10**9, bytes_accessed=6 * 10**6, transcendentals=0),
        compiler_params=pltpu.CompilerParams(vmem_limit_bytes=VMEM),
        name="project",
    )(scal, *gathered, w, wp)


def join_body(own_ref, other_ref, out_ref):
    out_ref[...] = (own_ref[...] + other_ref[...].astype(f32)).astype(bf16)


def join(own, other):
    length, width = own.shape
    rows = min(length, 1024)
    spec = pl.BlockSpec((rows, width), lambda i: (i, 0))
    return pl.pallas_call(
        join_body,
        grid=(length // rows,),
        in_specs=[spec, spec],
        out_specs=spec,
        out_shape=jax.ShapeDtypeStruct(own.shape, bf16),
        cost_estimate=pl.CostEstimate(flops=10**6, bytes_accessed=4 * 10**6, transcendentals=0),
        compiler_params=pltpu.CompilerParams(vmem_limit_bytes=VMEM),
        name="join",
    )(own, other)


def own_lanes(x, zn, sub, core):
    out = None
    for c in range(CORES):
        at = [(z * CORES + c) * sub for z in range(zn)]
        part = jnp.concatenate([x[:, a : a + sub] for a in at], axis=1)
        out = part if out is None else jnp.where(core == c, part, out)
    return out


def targets(idx, me, zn, experts, capacity):
    n = idx.shape[1]
    sub = n // zn
    lines = max(8, experts)
    line = lax.broadcasted_iota(jnp.int32, (lines, n), 0)
    picks = [line == idx[r : r + 1] for r in range(TOPK)]
    onehot = jnp.where(picks[0] | picks[1], 1.0, 0.0).astype(bf16)
    row = lax.broadcasted_iota(jnp.int32, (n, n), 0)
    col = lax.broadcasted_iota(jnp.int32, (n, n), 1)
    earlier = ((row < col) & (row // sub == col // sub)).astype(bf16)
    counts = mm(onehot, earlier)
    blk = lax.broadcasted_iota(jnp.int32, (1, n), 1) // sub
    out = []
    for r in range(TOPK):
        slot = jnp.sum(jnp.where(picks[r], counts, 0.0), axis=0, keepdims=True).astype(jnp.int32)
        out.append((idx[r : r + 1] ^ me) * (zn * capacity) + blk * capacity + slot)
    return out


def pack_body(experts, capacity, sc_ref, tok_ref, idx_ref, gain_ref, *outs):
    zn, _, sub, width = tok_ref.shape
    n = zn * sub
    x = tok_ref[...].reshape(n, width).astype(f32)
    x = (x * lax.rsqrt(jnp.mean(x * x, axis=1, keepdims=True) + epsilon) * gain_ref[...]).astype(bf16)
    t = targets(own_lanes(idx_ref[...], zn, sub, sc_ref[1]), sc_ref[0], zn, experts, capacity)
    per = zn * capacity
    line = lax.broadcasted_iota(jnp.int32, (per, n), 0)
    for m in range(experts):
        hit = (t[0] == line + m * per) | (t[1] == line + m * per)
        outs[m][...] = mm(jnp.where(hit, 1.0, 0.0).astype(bf16), x).astype(bf16)


def pack(scal, tokens, idx, gain, experts, capacity):
    zn, _, sub, width = tokens.shape
    shape = jax.ShapeDtypeStruct((zn * capacity, width), bf16)
    return pl.pallas_call(
        functools.partial(pack_body, experts, capacity),
        grid_spec=pltpu.PrefetchScalarGridSpec(
            num_scalar_prefetch=1,
            grid=(1,),
            in_specs=[
                pl.BlockSpec((zn, 1, sub, width), lambda i, s: (0, s[1], 0, 0)),
                pl.BlockSpec(idx.shape, lambda i, s: (0, 0)),
                pl.BlockSpec((1, width), lambda i, s: (0, 0)),
            ],
            out_specs=[pl.BlockSpec(shape.shape, lambda i, s: (0, 0))] * experts,
        ),
        out_shape=[shape] * experts,
        cost_estimate=pl.CostEstimate(flops=4 * 10**9, bytes_accessed=4 * 10**6, transcendentals=10**3),
        compiler_params=pltpu.CompilerParams(vmem_limit_bytes=VMEM),
        name="pack",
    )(scal, tokens, idx, gain.reshape(1, width))


def hidden_chunks(hidden):
    units, unit = (hidden // 128, 128) if hidden % 128 == 0 else (1, hidden)
    out, step = [], 1
    while units:
        take = min(step, units)
        if units - take < step:
            take = units
        out.append(take * unit)
        units -= take
        step *= 2
    return out


def ffn_body(count, pieces, chunks, *refs):
    xs = refs[:count]
    sources = refs[count : count + 6]
    outs = refs[count + 6 : count + 6 + count * pieces]
    scratch = refs[count + 6 + count * pieces :]
    x_ref, acc_ref, sems = scratch[0], scratch[1], scratch[2]
    buffers = scratch[3:]
    per = xs[0].shape[0]

    def copies(c):
        at = sum(chunks[:c])
        span = pl.ds(at, chunks[c])
        for k in range(3):
            for side in range(2):
                src = sources[2 * k + side].at[0]
                src = src.at[span, :] if k == 2 else src.at[:, span]
                yield pltpu.make_async_copy(src, buffers[3 * c + k].at[side], sems.at[c, 2 * k + side])

    for c in range(len(chunks)):
        for copy in copies(c):
            copy.start()
    x_ref[...] = jnp.concatenate([x[...] for x in xs], axis=0)
    for c in range(len(chunks)):
        for copy in copies(c):
            copy.wait()
        bg, bu, bd = buffers[3 * c : 3 * c + 3]
        x = x_ref[...]
        g = mm(x, jnp.concatenate([bg[0], bg[1]], axis=1))
        u = mm(x, jnp.concatenate([bu[0], bu[1]], axis=1))
        h = (g * sigmoid(g) * u).astype(bf16)
        part = mm(h, jnp.concatenate([bd[0], bd[1]], axis=0))
        if c == 0 and len(chunks) > 1:
            acc_ref[...] = part
        elif c + 1 < len(chunks):
            acc_ref[...] += part
        else:
            total = part if c == 0 else acc_ref[...] + part
            cols = total.shape[1] // pieces
            for i in range(count):
                for p in range(pieces):
                    piece = total[i * per : (i + 1) * per, p * cols : (p + 1) * cols]
                    outs[i * pieces + p][...] = piece.astype(bf16)


def ffn(xs, weights, pieces):
    count = len(xs)
    per, width = xs[0].shape
    hidden = weights[0].shape[2]
    chunks = hidden_chunks(hidden)
    buffers = []
    for c in chunks:
        buffers += [pltpu.VMEM((2, width, c), bf16), pltpu.VMEM((2, width, c), bf16), pltpu.VMEM((2, c, width), bf16)]
    whole = pl.BlockSpec((per, width), lambda: (0, 0))
    out = pl.BlockSpec((per, width // pieces), lambda: (0, 0))
    outs = pl.pallas_call(
        functools.partial(ffn_body, count, pieces, chunks),
        in_specs=[whole] * count + [pl.BlockSpec(memory_space=pl.ANY)] * 6,
        out_specs=[out] * (count * pieces),
        out_shape=[jax.ShapeDtypeStruct((per, width // pieces), bf16)] * (count * pieces),
        scratch_shapes=[
            pltpu.VMEM((count * per, width), bf16),
            pltpu.VMEM((count * per, width), f32),
            pltpu.SemaphoreType.DMA((len(chunks), 6)),
        ]
        + buffers,
        cost_estimate=pl.CostEstimate(flops=8 * 10**9, bytes_accessed=25 * 10**6, transcendentals=10**6),
        compiler_params=pltpu.CompilerParams(vmem_limit_bytes=FFN_VMEM),
        name="ffn",
    )(*xs, *weights)
    return [outs[i * pieces : (i + 1) * pieces] for i in range(count)]


def combine_body(experts, capacity, zn, sc_ref, idx_ref, w_ref, *refs):
    ys = refs[:experts]
    outs = refs[experts : experts + zn]
    acc_ref = refs[-1]
    sub = outs[0].shape[0]
    n = zn * sub
    t = targets(own_lanes(idx_ref[...], zn, sub, sc_ref[1]), sc_ref[0], zn, experts, capacity)
    w = own_lanes(w_ref[...], zn, sub, sc_ref[1])
    per = zn * capacity
    line = lax.broadcasted_iota(jnp.int32, (per, n), 0)
    acc = None
    for m in range(experts):
        c = jnp.where(t[0] == line + m * per, w[0:1], 0.0)
        c = c + jnp.where(t[1] == line + m * per, w[1:2], 0.0)
        part = mm(c.astype(bf16), ys[m][...], ((0,), (0,)))
        acc = part if acc is None else acc + part
    acc_ref[...] = acc.reshape(zn, sub, acc.shape[1]).astype(bf16)
    for m in range(zn):
        outs[m][...] = acc_ref[sc_ref[2] ^ m]


def combine(scal, idx, w, ys, piece, pieces, zn, sub, capacity):
    experts = len(ys)
    per = zn * capacity
    cols = ys[0].shape[1] // pieces if ys[0].shape[1] == max(y.shape[1] for y in ys) else ys[0].shape[1]
    shape = jax.ShapeDtypeStruct((sub, cols), bf16)
    return pl.pallas_call(
        functools.partial(combine_body, experts, capacity, zn),
        grid_spec=pltpu.PrefetchScalarGridSpec(
            num_scalar_prefetch=1,
            grid=(1,),
            in_specs=[pl.BlockSpec(idx.shape, lambda i, s: (0, 0))] * 2
            + [
                pl.BlockSpec((per, cols), (lambda i, s: (0, piece)) if y.shape[1] != cols else (lambda i, s: (0, 0)))
                for y in ys
            ],
            out_specs=[pl.BlockSpec(shape.shape, lambda i, s: (0, 0))] * zn,
            scratch_shapes=[pltpu.VMEM((zn, sub, cols), bf16)],
        ),
        out_shape=[shape] * zn,
        cost_estimate=pl.CostEstimate(flops=10**9, bytes_accessed=2 * 10**6, transcendentals=10**3),
        compiler_params=pltpu.CompilerParams(vmem_limit_bytes=VMEM),
        name="combine",
    )(scal, idx, w, *ys)


def on_device(
    query_preactivation,
    forget_preactivation,
    value_input_rows,
    output_gate_preactivation,
    forget_floor_gap,
    extra_log_forget,
    head_output_gain,
    mixer_output_weight,
    second_batch_tokens,
    feedforward_norm_gain,
    chosen_expert_index,
    chosen_expert_weight,
    expert_gate_weight,
    expert_up_weight,
    expert_down_weight,
):
    ep = lax.axis_size("ep")
    tp = lax.axis_size("tp")
    zn = tp // CORES
    me = lax.axis_index("ep").astype(jnp.int32)
    place = lax.axis_index("tp").astype(jnp.int32)
    zi, core = place >> 1, place & 1
    scal = jnp.stack([me, core, zi])
    over_ep = lambda x, m: lax.ppermute(x, "ep", [(i, i ^ m) for i in range(ep)])
    over_core = lambda x: lax.ppermute(x, "tp", [(i, i ^ 1) for i in range(tp)])
    over_z = lambda x, m: lax.ppermute(x, "tp", [(i, i ^ (m * CORES)) for i in range(tp)])
    tie = lax.optimization_barrier
    assert expert_gate_weight.shape[0] == 1
    experts = ep
    rows, width = second_batch_tokens.shape
    sub = rows // tp
    capacity = max(2, sub * TOPK * 5 // (4 * experts))
    pieces = PIECES
    extra = extra_log_forget.T
    idx = chosen_expert_index.T
    wts = chosen_expert_weight.T

    weights = []
    for w in (expert_gate_weight, expert_up_weight, expert_down_weight):
        weights += [w, over_core(w)]
    wp = over_core(mixer_output_weight)

    st = final_state(forget_preactivation, value_input_rows, forget_floor_gap, extra)
    states = [over_ep(st, m) for m in range(1, ep)]

    tokens, _ = tie((second_batch_tokens, st))
    tokens = tokens.reshape(zn, CORES, sub, width)
    packed = pack(scal, tokens, idx, feedforward_norm_gain, experts, capacity)
    order = [ep - 1] + list(range(1, ep - 1))
    arrived = {0: packed[0]}
    for m in order:
        arrived[m] = over_ep(packed[m], m)

    q, _ = tie((query_preactivation, packed[1]))
    mixed = mixer(
        scal,
        states,
        q,
        forget_preactivation,
        value_input_rows,
        output_gate_preactivation,
        forget_floor_gap,
        extra,
        head_output_gain,
    )
    gathered = [mixed]
    for m in range(1, zn):
        chained = m % 2 == 1 and m > 1
        gathered.append(over_z(gathered[m - 1] if chained else mixed, 1 if chained else m))

    x0, _ = tie((arrived[0], mixed))
    (y1,), (y0,) = ffn([arrived[ep - 1], x0], weights, 1)
    late = ffn([arrived[m] for m in order[1:]], weights, pieces)
    first_back = over_ep(y1, ep - 1)
    back = [[over_ep(late[i][p], m) for i, m in enumerate(order[1:])] for p in range(pieces)]
    own, other = project(scal, gathered, mixer_output_weight, wp)
    other = over_core(other)
    mixer_output_first = join(own, other)
    outs = []
    for p in range(pieces):
        ys = [y0] + back[p] + [first_back]
        parts = combine(scal, idx, wts, ys, p, pieces, zn, sub, capacity)
        total = parts[0].astype(f32)
        for m in range(1, zn):
            total = total + over_z(parts[m], m).astype(f32)
        outs.append(total.astype(bf16))
    return mixer_output_first, jnp.concatenate(outs, axis=1)


def solution(mesh):
    placed = (
        P("ep", "tp"),
        P("ep", "tp"),
        P("ep", "tp"),
        P("ep", "tp"),
        P("tp"),
        P("ep", "tp"),
        P("tp"),
        P(None, "tp"),
        P("ep", None),
        P(),
        P("ep", None),
        P("ep", None),
        P("ep", None, "tp"),
        P("ep", None, "tp"),
        P("ep", "tp", None),
    )

    return jax.shard_map(
        on_device,
        mesh=mesh,
        in_specs=placed,
        out_specs=(P("ep", "tp"), P(("ep", "tp"), None)),
        check_vma=False,
    )
```

```python
import functools
import jax
import jax.numpy as jnp
from jax import lax
from jax.experimental import pallas as pl
from jax.experimental.pallas import tpu as pltpu
from jax.sharding import PartitionSpec as P


KEY_DIM = 128
VAL_DIM = 64
BLOCK = 64
TOPK = 2
CORES = 2
PIECES = (2, 3, 3)
MIXER_ROWS = 2048
FFN_VMEM = 36 * 1024 * 1024
VMEM = 20 * 1024 * 1024
epsilon = 1e-06
f32 = jnp.float32
bf16 = jnp.bfloat16


def mm(a, b, dims=((1,), (0,))):
    return lax.dot_general(a, b, (dims, ((), ())), preferred_element_type=f32)


def split2(x):
    hi = x.astype(bf16)
    return hi, (x - hi.astype(f32)).astype(bf16)


def sigmoid(x):
    return 0.5 + 0.5 * jnp.tanh(0.5 * x)


def forget_log(heads, f, gap, extra):
    key = gap * sigmoid(-f.astype(f32))
    kw = heads * KEY_DIM
    pick = lax.broadcasted_iota(jnp.int32, (heads, kw), 1) // KEY_DIM
    pick = (pick == lax.broadcasted_iota(jnp.int32, (heads, kw), 0)).astype(bf16)
    hi, lo = split2(extra)
    extra = mm(hi, pick, ((0,), (0,))) + mm(lo, pick, ((0,), (0,)))
    return key, jnp.log(1.0 - key) + extra


def same_head(heads):
    shape = (heads * VAL_DIM, heads * KEY_DIM)
    vh = lax.broadcasted_iota(jnp.int32, shape, 0) // VAL_DIM
    return vh == lax.broadcasted_iota(jnp.int32, shape, 1) // KEY_DIM


def state_body(heads, rows, f_hbm, v_hbm, gap_hbm, extra_hbm, st_ref, f_ref, v_ref, gap_ref, extra_ref, sems):
    vw = heads * VAL_DIM
    kw = heads * KEY_DIM
    length = f_ref.shape[0]
    half = max(rows, length // 2)
    copies = [
        pltpu.make_async_copy(gap_hbm, gap_ref, sems.at[0]),
        pltpu.make_async_copy(extra_hbm, extra_ref, sems.at[1]),
    ]
    for n, at in enumerate(range(0, length, half)):
        span = pl.ds(at, half)
        copies.append(pltpu.make_async_copy(f_hbm.at[span], f_ref.at[span], sems.at[2 + 2 * n]))
        copies.append(pltpu.make_async_copy(v_hbm.at[span], v_ref.at[span], sems.at[3 + 2 * n]))
    for copy in copies:
        copy.start()
    row = lax.broadcasted_iota(jnp.int32, (rows, rows), 0)
    later = (row < lax.broadcasted_iota(jnp.int32, (rows, rows), 1)).astype(bf16)
    s = jnp.zeros((vw, kw), f32)
    l = jnp.zeros((1, kw), f32)
    copies[0].wait()
    copies[1].wait()
    for at in range(0, length, rows):
        if at % half == 0:
            copies[2 + 2 * (at // half)].wait()
            copies[3 + 2 * (at // half)].wait()
        rs = slice(at, at + rows)
        key, logf = forget_log(heads, f_ref[rs, :], gap_ref[...], extra_ref[:, rs])
        hi, lo = split2(logf)
        rest = mm(later, hi) + mm(later, lo)
        whole = rest[0:1] + logf[0:1]
        ks = (key * jnp.exp(rest)).astype(bf16)
        s = s * jnp.exp(whole) + mm(v_ref[rs, :], ks, ((0,), (0,)))
        l = l + whole
    for h in range(heads):
        st_ref[h * VAL_DIM : (h + 1) * VAL_DIM, :] = s[
            h * VAL_DIM : (h + 1) * VAL_DIM, h * KEY_DIM : (h + 1) * KEY_DIM
        ]
        st_ref[vw + h : vw + h + 1, :] = l[:, h * KEY_DIM : (h + 1) * KEY_DIM]


def final_state(f, v, gap, extra):
    length, kw = f.shape
    heads = kw // KEY_DIM
    vw = heads * VAL_DIM
    return pl.pallas_call(
        functools.partial(state_body, heads, 4 * BLOCK),
        in_specs=[pl.BlockSpec(memory_space=pltpu.HBM)] * 4,
        out_specs=pl.BlockSpec((vw + 8, KEY_DIM), lambda: (0, 0)),
        out_shape=jax.ShapeDtypeStruct((vw + 8, KEY_DIM), f32),
        scratch_shapes=[
            pltpu.VMEM((length, kw), bf16),
            pltpu.VMEM((length, vw), bf16),
            pltpu.VMEM((1, kw), f32),
            pltpu.VMEM(extra.shape, f32),
            pltpu.SemaphoreType.DMA((6,)),
        ],
        cost_estimate=pl.CostEstimate(flops=4 * 10**9, bytes_accessed=2 * 10**6, transcendentals=10**6),
        name="final_state",
    )(f, v, gap.reshape(1, kw), extra)


def mixer_body(heads, ep, rows, sc_ref, *refs):
    others = refs[: ep - 1]
    q_ref, f_ref, v_ref, gate_ref, gap_ref, extra_ref, gain_ref, mixed_ref, s_ref = refs[ep - 1 :]
    kw = heads * KEY_DIM
    vw = heads * VAL_DIM
    blocks = rows // BLOCK
    me = sc_ref[0]

    @pl.when(pl.program_id(0) == 0)
    def _():
        carried = [jnp.zeros((VAL_DIM, KEY_DIM), f32) for _ in range(heads)]
        for j in range(ep):
            use = j < me
            for m in range(1, ep):
                flag = jnp.where(use & ((me ^ m) == j), 1.0, 0.0).astype(f32)
                o = others[m - 1]
                for h in range(heads):
                    decay = jnp.exp(o[vw + h : vw + h + 1, :] * flag)
                    carried[h] = carried[h] * decay + o[h * VAL_DIM : (h + 1) * VAL_DIM, :] * flag
        s_ref[...] = jnp.zeros_like(s_ref)
        for h in range(heads):
            s_ref[h * VAL_DIM : (h + 1) * VAL_DIM, h * KEY_DIM : (h + 1) * KEY_DIM] = carried[h]

    row = lax.broadcasted_iota(jnp.int32, (rows, rows), 0)
    col = lax.broadcasted_iota(jnp.int32, (rows, rows), 1)
    causal = (row >= col) & (row // BLOCK == col // BLOCK)
    tri = causal.astype(bf16)
    same = same_head(heads)
    a = lax.broadcasted_iota(jnp.int32, (vw, vw), 0) // VAL_DIM
    b = lax.broadcasted_iota(jnp.int32, (vw, vw), 1) // VAL_DIM
    ones = (a == b).astype(bf16)
    s = s_ref[...]
    for at in range(0, q_ref.shape[0], rows):
        part = slice(at, at + rows)
        q = q_ref[part, :].astype(f32)
        q = q * sigmoid(q)
        key, logf = forget_log(heads, f_ref[part, :], gap_ref[...], extra_ref[:, part])
        hi, lo = split2(logf)
        cum = mm(tri, hi) + mm(tri, lo)
        v = v_ref[part, :]
        finals = [cum[(b + 1) * BLOCK - 1 : (b + 1) * BLOCK] for b in range(blocks)]
        fin = jnp.concatenate([jnp.broadcast_to(x, (BLOCK, kw)) for x in finals], axis=0)
        qs = (q * jnp.exp(cum - fin)).astype(bf16)
        ks = (key * jnp.exp(fin - cum)).astype(bf16)
        qc = (q * jnp.exp(cum)).astype(bf16)
        within = []
        for h in range(heads):
            ksl = slice(h * KEY_DIM, (h + 1) * KEY_DIM)
            sc = mm(qs[:, ksl], ks[:, ksl], ((1,), (1,)))
            sc = jnp.where(causal, sc, 0.0).astype(bf16)
            within.append(mm(sc, v[:, h * VAL_DIM : (h + 1) * VAL_DIM]))
        within = jnp.concatenate(within, axis=1)
        across = []
        for b in range(blocks):
            rs = slice(b * BLOCK, (b + 1) * BLOCK)
            across.append(mm(qc[rs], s.astype(bf16), ((1,), (1,))))
            upd = jnp.where(same, mm(v[rs], ks[rs], ((0,), (0,))), 0.0)
            s = s * jnp.exp(finals[b]) + upd
        rec = within + jnp.concatenate(across, axis=0)
        hi, lo = split2(rec * rec)
        mean = (mm(hi, ones) + mm(lo, ones)) * (1.0 / VAL_DIM)
        g = gate_ref[part, :].astype(f32)
        mixed_ref[part, :] = (
            rec * lax.rsqrt(mean + epsilon) * gain_ref[...] * (g * sigmoid(g))
        ).astype(bf16)
    s_ref[...] = s


def mixer(scal, others, q, f, v, gate, gap, extra, gain):
    length, kw = q.shape
    heads = kw // KEY_DIM
    vw = heads * VAL_DIM
    ep = len(others) + 1
    rows = min(length, MIXER_ROWS)
    rows_of = lambda w: pl.BlockSpec((rows, w), lambda i, s: (i, 0))
    whole = lambda r, w: pl.BlockSpec((r, w), lambda i, s: (0, 0))
    return pl.pallas_call(
        functools.partial(mixer_body, heads, ep, 4 * BLOCK),
        grid_spec=pltpu.PrefetchScalarGridSpec(
            num_scalar_prefetch=1,
            grid=(length // rows,),
            in_specs=[whole(vw + 8, KEY_DIM)] * (ep - 1)
            + [rows_of(kw), rows_of(kw), rows_of(vw), rows_of(vw), whole(1, kw)]
            + [pl.BlockSpec((heads, rows), lambda i, s: (0, i)), whole(1, vw)],
            out_specs=rows_of(vw),
            scratch_shapes=[pltpu.VMEM((vw, kw), f32)],
        ),
        out_shape=jax.ShapeDtypeStruct((length, vw), bf16),
        cost_estimate=pl.CostEstimate(flops=12 * 10**9, bytes_accessed=4 * 10**6, transcendentals=10**6),
        compiler_params=pltpu.CompilerParams(vmem_limit_bytes=VMEM),
        name="mixer",
    )(scal, *others, q, f, v, gate, gap.reshape(1, kw), extra, gain.reshape(1, vw))


def project_body(zn, sc_ref, *refs):
    gs = refs[:zn]
    w_ref, wp_ref, own_ref, other_ref = refs[zn:]
    vw = gs[0].shape[1]
    own = other = None
    for m in range(zn):
        at = pl.multiple_of(((sc_ref[2] ^ m) * CORES + sc_ref[1]) * vw, vw)
        g = gs[m][...]
        a = mm(g, w_ref[pl.ds(at, vw), :])
        b = mm(g, wp_ref[pl.ds(at, vw), :])
        own = a if own is None else own + a
        other = b if other is None else other + b
    own_ref[...] = own
    other_ref[...] = other.astype(bf16)


def project(scal, gathered, w, wp):
    length, vw = gathered[0].shape
    zn = len(gathered)
    rows = min(length, 1024)
    rows_of = lambda n: pl.BlockSpec((rows, n), lambda i, s: (i, 0))
    whole = pl.BlockSpec(w.shape, lambda i, s: (0, 0))
    width = w.shape[1]
    return pl.pallas_call(
        functools.partial(project_body, zn),
        grid_spec=pltpu.PrefetchScalarGridSpec(
            num_scalar_prefetch=1,
            grid=(length // rows,),
            in_specs=[rows_of(vw)] * zn + [whole, whole],
            out_specs=[rows_of(width), rows_of(width)],
        ),
        out_shape=[
            jax.ShapeDtypeStruct((length, width), f32),
            jax.ShapeDtypeStruct((length, width), bf16),
        ],
        cost_estimate=pl.CostEstimate(flops=2 * 10**9, bytes_accessed=6 * 10**6, transcendentals=0),
        compiler_params=pltpu.CompilerParams(vmem_limit_bytes=VMEM),
        name="project",
    )(scal, *gathered, w, wp)


def join_body(own_ref, other_ref, out_ref):
    out_ref[...] = (own_ref[...] + other_ref[...].astype(f32)).astype(bf16)


def join(own, other):
    length, width = own.shape
    rows = min(length, 1024)
    spec = pl.BlockSpec((rows, width), lambda i: (i, 0))
    return pl.pallas_call(
        join_body,
        grid=(length // rows,),
        in_specs=[spec, spec],
        out_specs=spec,
        out_shape=jax.ShapeDtypeStruct(own.shape, bf16),
        cost_estimate=pl.CostEstimate(flops=10**6, bytes_accessed=4 * 10**6, transcendentals=0),
        compiler_params=pltpu.CompilerParams(vmem_limit_bytes=VMEM),
        name="join",
    )(own, other)


def own_lanes(x, zn, sub, core):
    out = None
    for c in range(CORES):
        at = [(z * CORES + c) * sub for z in range(zn)]
        part = jnp.concatenate([x[:, a : a + sub] for a in at], axis=1)
        out = part if out is None else jnp.where(core == c, part, out)
    return out


def targets(idx, me, zn, experts, capacity):
    n = idx.shape[1]
    sub = n // zn
    lines = max(8, experts)
    line = lax.broadcasted_iota(jnp.int32, (lines, n), 0)
    picks = [line == idx[r : r + 1] for r in range(TOPK)]
    onehot = jnp.where(picks[0] | picks[1], 1.0, 0.0).astype(bf16)
    row = lax.broadcasted_iota(jnp.int32, (n, n), 0)
    col = lax.broadcasted_iota(jnp.int32, (n, n), 1)
    earlier = ((row < col) & (row // sub == col // sub)).astype(bf16)
    counts = mm(onehot, earlier)
    blk = lax.broadcasted_iota(jnp.int32, (1, n), 1) // sub
    out = []
    for r in range(TOPK):
        slot = jnp.sum(jnp.where(picks[r], counts, 0.0), axis=0, keepdims=True).astype(jnp.int32)
        out.append((idx[r : r + 1] ^ me) * (zn * capacity) + blk * capacity + slot)
    return out


def pack_body(experts, capacity, sc_ref, tok_ref, idx_ref, gain_ref, *outs):
    zn, _, sub, width = tok_ref.shape
    n = zn * sub
    x = tok_ref[...].reshape(n, width).astype(f32)
    x = (x * lax.rsqrt(jnp.mean(x * x, axis=1, keepdims=True) + epsilon) * gain_ref[...]).astype(bf16)
    t = targets(own_lanes(idx_ref[...], zn, sub, sc_ref[1]), sc_ref[0], zn, experts, capacity)
    per = zn * capacity
    line = lax.broadcasted_iota(jnp.int32, (per, n), 0)
    for m in range(experts):
        hit = (t[0] == line + m * per) | (t[1] == line + m * per)
        outs[m][...] = mm(jnp.where(hit, 1.0, 0.0).astype(bf16), x).astype(bf16)


def pack(scal, tokens, idx, gain, experts, capacity):
    zn, _, sub, width = tokens.shape
    shape = jax.ShapeDtypeStruct((zn * capacity, width), bf16)
    return pl.pallas_call(
        functools.partial(pack_body, experts, capacity),
        grid_spec=pltpu.PrefetchScalarGridSpec(
            num_scalar_prefetch=1,
            grid=(1,),
            in_specs=[
                pl.BlockSpec((zn, 1, sub, width), lambda i, s: (0, s[1], 0, 0)),
                pl.BlockSpec(idx.shape, lambda i, s: (0, 0)),
                pl.BlockSpec((1, width), lambda i, s: (0, 0)),
            ],
            out_specs=[pl.BlockSpec(shape.shape, lambda i, s: (0, 0))] * experts,
        ),
        out_shape=[shape] * experts,
        cost_estimate=pl.CostEstimate(flops=4 * 10**9, bytes_accessed=4 * 10**6, transcendentals=10**3),
        compiler_params=pltpu.CompilerParams(vmem_limit_bytes=VMEM),
        name="pack",
    )(scal, tokens, idx, gain.reshape(1, width))


def hidden_chunks(hidden):
    units, unit = (hidden // 128, 128) if hidden % 128 == 0 else (1, hidden)
    out, step = [], 1
    while units:
        take = min(step, units)
        if units - take < step:
            take = units
        out.append(take * unit)
        units -= take
        step *= 2
    return out


def ffn_body(count, pieces, chunks, *refs):
    xs = refs[:count]
    sources = refs[count : count + 6]
    outs = refs[count + 6 : count + 6 + count * len(pieces)]
    scratch = refs[count + 6 + count * len(pieces) :]
    x_ref, acc_ref, sems = scratch[0], scratch[1], scratch[2]
    buffers = scratch[3:]
    per = xs[0].shape[0]

    def copies(c):
        at = sum(chunks[:c])
        span = pl.ds(at, chunks[c])
        for k in range(3):
            for side in range(2):
                src = sources[2 * k + side].at[0]
                src = src.at[span, :] if k == 2 else src.at[:, span]
                yield pltpu.make_async_copy(src, buffers[3 * c + k].at[side], sems.at[c, 2 * k + side])

    for c in range(len(chunks)):
        for copy in copies(c):
            copy.start()
    x_ref[...] = jnp.concatenate([x[...] for x in xs], axis=0)
    for c in range(len(chunks)):
        for copy in copies(c):
            copy.wait()
        bg, bu, bd = buffers[3 * c : 3 * c + 3]
        x = x_ref[...]
        g = mm(x, jnp.concatenate([bg[0], bg[1]], axis=1))
        u = mm(x, jnp.concatenate([bu[0], bu[1]], axis=1))
        h = (g * sigmoid(g) * u).astype(bf16)
        part = mm(h, jnp.concatenate([bd[0], bd[1]], axis=0))
        if c == 0 and len(chunks) > 1:
            acc_ref[...] = part
        elif c + 1 < len(chunks):
            acc_ref[...] += part
        else:
            total = part if c == 0 else acc_ref[...] + part
            for i in range(count):
                for p, (left, right) in enumerate(pieces):
                    outs[i * len(pieces) + p][...] = total[i * per : (i + 1) * per, left:right].astype(bf16)


def ffn(xs, weights, pieces):
    count = len(xs)
    per, width = xs[0].shape
    hidden = weights[0].shape[2]
    chunks = hidden_chunks(hidden)
    buffers = []
    for c in chunks:
        buffers += [pltpu.VMEM((2, width, c), bf16), pltpu.VMEM((2, width, c), bf16), pltpu.VMEM((2, c, width), bf16)]
    whole = pl.BlockSpec((per, width), lambda: (0, 0))
    widths = [right - left for left, right in pieces]
    outs = pl.pallas_call(
        functools.partial(ffn_body, count, pieces, chunks),
        in_specs=[whole] * count + [pl.BlockSpec(memory_space=pl.ANY)] * 6,
        out_specs=[pl.BlockSpec((per, w), lambda: (0, 0)) for w in widths] * count,
        out_shape=[jax.ShapeDtypeStruct((per, w), bf16) for w in widths] * count,
        scratch_shapes=[
            pltpu.VMEM((count * per, width), bf16),
            pltpu.VMEM((count * per, width), f32),
            pltpu.SemaphoreType.DMA((len(chunks), 6)),
        ]
        + buffers,
        cost_estimate=pl.CostEstimate(flops=8 * 10**9, bytes_accessed=25 * 10**6, transcendentals=10**6),
        compiler_params=pltpu.CompilerParams(vmem_limit_bytes=FFN_VMEM),
        name="ffn",
    )(*xs, *weights)
    n = len(pieces)
    return [outs[i * n : (i + 1) * n] for i in range(count)]


def combine_body(experts, capacity, zn, lefts, cols, sc_ref, idx_ref, w_ref, *refs):
    ys = refs[:experts]
    outs = refs[experts : experts + zn]
    acc_ref = refs[-1]
    sub = outs[0].shape[0]
    n = zn * sub
    t = targets(own_lanes(idx_ref[...], zn, sub, sc_ref[1]), sc_ref[0], zn, experts, capacity)
    w = own_lanes(w_ref[...], zn, sub, sc_ref[1])
    per = zn * capacity
    line = lax.broadcasted_iota(jnp.int32, (per, n), 0)
    acc = None
    for m in range(experts):
        c = jnp.where(t[0] == line + m * per, w[0:1], 0.0)
        c = c + jnp.where(t[1] == line + m * per, w[1:2], 0.0)
        y = ys[m][:, lefts[m] : lefts[m] + cols]
        part = mm(c.astype(bf16), y, ((0,), (0,)))
        acc = part if acc is None else acc + part
    acc_ref[...] = acc.reshape(zn, sub, acc.shape[1]).astype(bf16)
    for m in range(zn):
        outs[m][...] = acc_ref[sc_ref[2] ^ m]


def combine(scal, idx, w, ys, lefts, cols, zn, sub, capacity):
    experts = len(ys)
    shape = jax.ShapeDtypeStruct((sub, cols), bf16)
    whole = lambda shape: pl.BlockSpec(shape, lambda i, s: (0, 0))
    return pl.pallas_call(
        functools.partial(combine_body, experts, capacity, zn, lefts, cols),
        grid_spec=pltpu.PrefetchScalarGridSpec(
            num_scalar_prefetch=1,
            grid=(1,),
            in_specs=[whole(idx.shape)] * 2 + [whole(y.shape) for y in ys],
            out_specs=[whole(shape.shape)] * zn,
            scratch_shapes=[pltpu.VMEM((zn, sub, cols), bf16)],
        ),
        out_shape=[shape] * zn,
        cost_estimate=pl.CostEstimate(flops=10**9, bytes_accessed=2 * 10**6, transcendentals=10**3),
        compiler_params=pltpu.CompilerParams(vmem_limit_bytes=VMEM),
        name="combine",
    )(scal, idx, w, *ys)


def columns(width, shares):
    units, out, left = width // 128, [], 0
    for p in range(len(shares)):
        right = units * sum(shares[: p + 1]) // sum(shares) * 128
        out.append((left, right))
        left = right
    return out


def on_device(
    query_preactivation,
    forget_preactivation,
    value_input_rows,
    output_gate_preactivation,
    forget_floor_gap,
    extra_log_forget,
    head_output_gain,
    mixer_output_weight,
    second_batch_tokens,
    feedforward_norm_gain,
    chosen_expert_index,
    chosen_expert_weight,
    expert_gate_weight,
    expert_up_weight,
    expert_down_weight,
):
    ep = lax.axis_size("ep")
    tp = lax.axis_size("tp")
    zn = tp // CORES
    me = lax.axis_index("ep").astype(jnp.int32)
    place = lax.axis_index("tp").astype(jnp.int32)
    zi, core = place >> 1, place & 1
    scal = jnp.stack([me, core, zi])
    over_ep = lambda x, m: lax.ppermute(x, "ep", [(i, i ^ m) for i in range(ep)])
    over_core = lambda x: lax.ppermute(x, "tp", [(i, i ^ 1) for i in range(tp)])
    over_z = lambda x, m: lax.ppermute(x, "tp", [(i, i ^ (m * CORES)) for i in range(tp)])
    tie = lax.optimization_barrier
    assert expert_gate_weight.shape[0] == 1
    experts = ep
    rows, width = second_batch_tokens.shape
    sub = rows // tp
    capacity = max(2, sub * TOPK * 5 // (4 * experts))
    cuts = columns(width, PIECES)
    pieces = len(cuts)
    extra = extra_log_forget.T
    idx = chosen_expert_index.T
    wts = chosen_expert_weight.T

    weights = []
    for w in (expert_gate_weight, expert_up_weight, expert_down_weight):
        weights += [w, over_core(w)]
    wp = over_core(mixer_output_weight)

    st = final_state(forget_preactivation, value_input_rows, forget_floor_gap, extra)
    states = [over_ep(st, m) for m in range(1, ep)]

    tokens, _ = tie((second_batch_tokens, st))
    tokens = tokens.reshape(zn, CORES, sub, width)
    packed = pack(scal, tokens, idx, feedforward_norm_gain, experts, capacity)
    order = [ep - 1] + list(range(1, ep - 1))
    arrived = {0: packed[0]}
    for m in order:
        arrived[m] = over_ep(packed[m], m)

    q, _ = tie((query_preactivation, packed[1]))
    mixed = mixer(
        scal,
        states,
        q,
        forget_preactivation,
        value_input_rows,
        output_gate_preactivation,
        forget_floor_gap,
        extra,
        head_output_gain,
    )
    gathered = [mixed]
    for m in range(1, zn):
        chained = m % 2 == 1 and m > 1
        gathered.append(over_z(gathered[m - 1] if chained else mixed, 1 if chained else m))

    x0, _ = tie((arrived[0], mixed))
    (y1,), (y0,) = ffn([arrived[ep - 1], x0], weights, [(0, width)])
    late = ffn([arrived[m] for m in order[1:]], weights, cuts)
    first_back = over_ep(y1, ep - 1)
    back = [[over_ep(late[i][p], m) for i, m in enumerate(order[1:])] for p in range(pieces)]
    own, other = project(scal, gathered, mixer_output_weight, wp)
    other = over_core(other)
    mixer_output_first = join(own, other)
    outs = []
    for p in range(pieces):
        ys = [y0] + back[p] + [first_back]
        left, right = cuts[p]
        lefts = [left] + [0] * (ep - 2) + [left]
        parts = combine(scal, idx, wts, ys, lefts, right - left, zn, sub, capacity)
        total = parts[0].astype(f32)
        for m in range(1, zn):
            total = total + over_z(parts[m], m).astype(f32)
        outs.append(total.astype(bf16))
    return mixer_output_first, jnp.concatenate(outs, axis=1)


def solution(mesh):
    placed = (
        P("ep", "tp"),
        P("ep", "tp"),
        P("ep", "tp"),
        P("ep", "tp"),
        P("tp"),
        P("ep", "tp"),
        P("tp"),
        P(None, "tp"),
        P("ep", None),
        P(),
        P("ep", None),
        P("ep", None),
        P("ep", None, "tp"),
        P("ep", None, "tp"),
        P("ep", "tp", None),
    )

    return jax.shard_map(
        on_device,
        mesh=mesh,
        in_specs=placed,
        out_specs=(P("ep", "tp"), P(("ep", "tp"), None)),
        check_vma=False,
    )
```

```python
import functools
import jax
import jax.numpy as jnp
from jax import lax
from jax.experimental import pallas as pl
from jax.experimental.pallas import tpu as pltpu
from jax.sharding import PartitionSpec as P


KEY_DIM = 128
VAL_DIM = 64
BLOCK = 64
TOPK = 2
CORES = 2
PIECES = (2, 3, 3)
STATE_GROUP = 4
MIXER_ROWS = 2048
FFN_VMEM = 36 * 1024 * 1024
VMEM = 20 * 1024 * 1024
epsilon = 1e-06
f32 = jnp.float32
bf16 = jnp.bfloat16


def mm(a, b, dims=((1,), (0,))):
    return lax.dot_general(a, b, (dims, ((), ())), preferred_element_type=f32)


def split2(x):
    hi = x.astype(bf16)
    return hi, (x - hi.astype(f32)).astype(bf16)


def sigmoid(x):
    return 0.5 + 0.5 * jnp.tanh(0.5 * x)


def forget_log(heads, f, gap, extra):
    key = gap * sigmoid(-f.astype(f32))
    kw = heads * KEY_DIM
    pick = lax.broadcasted_iota(jnp.int32, (heads, kw), 1) // KEY_DIM
    pick = (pick == lax.broadcasted_iota(jnp.int32, (heads, kw), 0)).astype(bf16)
    hi, lo = split2(extra)
    extra = mm(hi, pick, ((0,), (0,))) + mm(lo, pick, ((0,), (0,)))
    return key, jnp.log(1.0 - key) + extra


def same_head(heads):
    shape = (heads * VAL_DIM, heads * KEY_DIM)
    vh = lax.broadcasted_iota(jnp.int32, shape, 0) // VAL_DIM
    return vh == lax.broadcasted_iota(jnp.int32, shape, 1) // KEY_DIM


def state_body(heads, rows, f_hbm, v_hbm, gap_hbm, extra_hbm, st_ref, f_ref, v_ref, gap_ref, extra_ref, sems):
    vw = heads * VAL_DIM
    kw = heads * KEY_DIM
    length = f_ref.shape[0]
    half = max(rows, length // 2)
    copies = [
        pltpu.make_async_copy(gap_hbm, gap_ref, sems.at[0]),
        pltpu.make_async_copy(extra_hbm, extra_ref, sems.at[1]),
    ]
    for n, at in enumerate(range(0, length, half)):
        span = pl.ds(at, half)
        copies.append(pltpu.make_async_copy(f_hbm.at[span], f_ref.at[span], sems.at[2 + 2 * n]))
        copies.append(pltpu.make_async_copy(v_hbm.at[span], v_ref.at[span], sems.at[3 + 2 * n]))
    for copy in copies:
        copy.start()
    row = lax.broadcasted_iota(jnp.int32, (rows, rows), 0)
    later = (row < lax.broadcasted_iota(jnp.int32, (rows, rows), 1)).astype(bf16)
    s = jnp.zeros((vw, kw), f32)
    l = jnp.zeros((1, kw), f32)
    parts = []
    copies[0].wait()
    copies[1].wait()
    for at in range(0, length, rows):
        if at % half == 0:
            copies[2 + 2 * (at // half)].wait()
            copies[3 + 2 * (at // half)].wait()
        rs = slice(at, at + rows)
        key, logf = forget_log(heads, f_ref[rs, :], gap_ref[...], extra_ref[:, rs])
        hi, lo = split2(logf)
        parts.append((rs, key, logf[0:1], mm(later, hi) + mm(later, lo)))
        if len(parts) < STATE_GROUP and at + rows < length:
            continue
        for rs, key, first, rest in parts:
            whole = rest[0:1] + first
            ks = (key * jnp.exp(rest)).astype(bf16)
            s = s * jnp.exp(whole) + mm(v_ref[rs, :], ks, ((0,), (0,)))
            l = l + whole
        parts = []
    for h in range(heads):
        st_ref[h * VAL_DIM : (h + 1) * VAL_DIM, :] = s[
            h * VAL_DIM : (h + 1) * VAL_DIM, h * KEY_DIM : (h + 1) * KEY_DIM
        ]
        st_ref[vw + h : vw + h + 1, :] = l[:, h * KEY_DIM : (h + 1) * KEY_DIM]


def final_state(f, v, gap, extra):
    length, kw = f.shape
    heads = kw // KEY_DIM
    vw = heads * VAL_DIM
    return pl.pallas_call(
        functools.partial(state_body, heads, 4 * BLOCK),
        in_specs=[pl.BlockSpec(memory_space=pltpu.HBM)] * 4,
        out_specs=pl.BlockSpec((vw + 8, KEY_DIM), lambda: (0, 0)),
        out_shape=jax.ShapeDtypeStruct((vw + 8, KEY_DIM), f32),
        scratch_shapes=[
            pltpu.VMEM((length, kw), bf16),
            pltpu.VMEM((length, vw), bf16),
            pltpu.VMEM((1, kw), f32),
            pltpu.VMEM(extra.shape, f32),
            pltpu.SemaphoreType.DMA((6,)),
        ],
        cost_estimate=pl.CostEstimate(flops=4 * 10**9, bytes_accessed=2 * 10**6, transcendentals=10**6),
        name="final_state",
    )(f, v, gap.reshape(1, kw), extra)


def mixer_body(heads, ep, rows, sc_ref, *refs):
    others = refs[: ep - 1]
    q_ref, f_ref, v_ref, gate_ref, gap_ref, extra_ref, gain_ref, mixed_ref, s_ref = refs[ep - 1 :]
    kw = heads * KEY_DIM
    vw = heads * VAL_DIM
    blocks = rows // BLOCK
    me = sc_ref[0]

    @pl.when(pl.program_id(0) == 0)
    def _():
        carried = [jnp.zeros((VAL_DIM, KEY_DIM), f32) for _ in range(heads)]
        for j in range(ep):
            use = j < me
            for m in range(1, ep):
                flag = jnp.where(use & ((me ^ m) == j), 1.0, 0.0).astype(f32)
                o = others[m - 1]
                for h in range(heads):
                    decay = jnp.exp(o[vw + h : vw + h + 1, :] * flag)
                    carried[h] = carried[h] * decay + o[h * VAL_DIM : (h + 1) * VAL_DIM, :] * flag
        s_ref[...] = jnp.zeros_like(s_ref)
        for h in range(heads):
            s_ref[h * VAL_DIM : (h + 1) * VAL_DIM, h * KEY_DIM : (h + 1) * KEY_DIM] = carried[h]

    row = lax.broadcasted_iota(jnp.int32, (rows, rows), 0)
    col = lax.broadcasted_iota(jnp.int32, (rows, rows), 1)
    causal = (row >= col) & (row // BLOCK == col // BLOCK)
    tri = causal.astype(bf16)
    same = same_head(heads)
    a = lax.broadcasted_iota(jnp.int32, (vw, vw), 0) // VAL_DIM
    b = lax.broadcasted_iota(jnp.int32, (vw, vw), 1) // VAL_DIM
    ones = (a == b).astype(bf16)
    s = s_ref[...]
    for at in range(0, q_ref.shape[0], rows):
        part = slice(at, at + rows)
        q = q_ref[part, :].astype(f32)
        q = q * sigmoid(q)
        key, logf = forget_log(heads, f_ref[part, :], gap_ref[...], extra_ref[:, part])
        hi, lo = split2(logf)
        cum = mm(tri, hi) + mm(tri, lo)
        v = v_ref[part, :]
        finals = [cum[(b + 1) * BLOCK - 1 : (b + 1) * BLOCK] for b in range(blocks)]
        fin = jnp.concatenate([jnp.broadcast_to(x, (BLOCK, kw)) for x in finals], axis=0)
        qs = (q * jnp.exp(cum - fin)).astype(bf16)
        ks = (key * jnp.exp(fin - cum)).astype(bf16)
        qc = (q * jnp.exp(cum)).astype(bf16)
        within = []
        for h in range(heads):
            ksl = slice(h * KEY_DIM, (h + 1) * KEY_DIM)
            sc = mm(qs[:, ksl], ks[:, ksl], ((1,), (1,)))
            sc = jnp.where(causal, sc, 0.0).astype(bf16)
            within.append(mm(sc, v[:, h * VAL_DIM : (h + 1) * VAL_DIM]))
        within = jnp.concatenate(within, axis=1)
        across = []
        for b in range(blocks):
            rs = slice(b * BLOCK, (b + 1) * BLOCK)
            across.append(mm(qc[rs], s.astype(bf16), ((1,), (1,))))
            upd = jnp.where(same, mm(v[rs], ks[rs], ((0,), (0,))), 0.0)
            s = s * jnp.exp(finals[b]) + upd
        rec = within + jnp.concatenate(across, axis=0)
        hi, lo = split2(rec * rec)
        mean = (mm(hi, ones) + mm(lo, ones)) * (1.0 / VAL_DIM)
        g = gate_ref[part, :].astype(f32)
        mixed_ref[part, :] = (
            rec * lax.rsqrt(mean + epsilon) * gain_ref[...] * (g * sigmoid(g))
        ).astype(bf16)
    s_ref[...] = s


def mixer(scal, others, q, f, v, gate, gap, extra, gain):
    length, kw = q.shape
    heads = kw // KEY_DIM
    vw = heads * VAL_DIM
    ep = len(others) + 1
    rows = min(length, MIXER_ROWS)
    rows_of = lambda w: pl.BlockSpec((rows, w), lambda i, s: (i, 0))
    whole = lambda r, w: pl.BlockSpec((r, w), lambda i, s: (0, 0))
    return pl.pallas_call(
        functools.partial(mixer_body, heads, ep, 4 * BLOCK),
        grid_spec=pltpu.PrefetchScalarGridSpec(
            num_scalar_prefetch=1,
            grid=(length // rows,),
            in_specs=[whole(vw + 8, KEY_DIM)] * (ep - 1)
            + [rows_of(kw), rows_of(kw), rows_of(vw), rows_of(vw), whole(1, kw)]
            + [pl.BlockSpec((heads, rows), lambda i, s: (0, i)), whole(1, vw)],
            out_specs=rows_of(vw),
            scratch_shapes=[pltpu.VMEM((vw, kw), f32)],
        ),
        out_shape=jax.ShapeDtypeStruct((length, vw), bf16),
        cost_estimate=pl.CostEstimate(flops=12 * 10**9, bytes_accessed=4 * 10**6, transcendentals=10**6),
        compiler_params=pltpu.CompilerParams(vmem_limit_bytes=VMEM),
        name="mixer",
    )(scal, *others, q, f, v, gate, gap.reshape(1, kw), extra, gain.reshape(1, vw))


def project_body(zn, sc_ref, *refs):
    gs = refs[:zn]
    w_ref, wp_ref, own_ref, other_ref = refs[zn:]
    vw = gs[0].shape[1]
    own = other = None
    for m in range(zn):
        at = pl.multiple_of(((sc_ref[2] ^ m) * CORES + sc_ref[1]) * vw, vw)
        g = gs[m][...]
        a = mm(g, w_ref[pl.ds(at, vw), :])
        b = mm(g, wp_ref[pl.ds(at, vw), :])
        own = a if own is None else own + a
        other = b if other is None else other + b
    own_ref[...] = own
    other_ref[...] = other.astype(bf16)


def project(scal, gathered, w, wp):
    length, vw = gathered[0].shape
    zn = len(gathered)
    rows = min(length, 1024)
    rows_of = lambda n: pl.BlockSpec((rows, n), lambda i, s: (i, 0))
    whole = pl.BlockSpec(w.shape, lambda i, s: (0, 0))
    width = w.shape[1]
    return pl.pallas_call(
        functools.partial(project_body, zn),
        grid_spec=pltpu.PrefetchScalarGridSpec(
            num_scalar_prefetch=1,
            grid=(length // rows,),
            in_specs=[rows_of(vw)] * zn + [whole, whole],
            out_specs=[rows_of(width), rows_of(width)],
        ),
        out_shape=[
            jax.ShapeDtypeStruct((length, width), f32),
            jax.ShapeDtypeStruct((length, width), bf16),
        ],
        cost_estimate=pl.CostEstimate(flops=2 * 10**9, bytes_accessed=6 * 10**6, transcendentals=0),
        compiler_params=pltpu.CompilerParams(vmem_limit_bytes=VMEM),
        name="project",
    )(scal, *gathered, w, wp)


def join_body(own_ref, other_ref, out_ref):
    out_ref[...] = (own_ref[...] + other_ref[...].astype(f32)).astype(bf16)


def join(own, other):
    length, width = own.shape
    rows = min(length, 1024)
    spec = pl.BlockSpec((rows, width), lambda i: (i, 0))
    return pl.pallas_call(
        join_body,
        grid=(length // rows,),
        in_specs=[spec, spec],
        out_specs=spec,
        out_shape=jax.ShapeDtypeStruct(own.shape, bf16),
        cost_estimate=pl.CostEstimate(flops=10**6, bytes_accessed=4 * 10**6, transcendentals=0),
        compiler_params=pltpu.CompilerParams(vmem_limit_bytes=VMEM),
        name="join",
    )(own, other)


def own_lanes(x, zn, sub, core):
    out = None
    for c in range(CORES):
        at = [(z * CORES + c) * sub for z in range(zn)]
        part = jnp.concatenate([x[:, a : a + sub] for a in at], axis=1)
        out = part if out is None else jnp.where(core == c, part, out)
    return out


def targets(idx, me, zn, experts, capacity):
    n = idx.shape[1]
    sub = n // zn
    lines = max(8, experts)
    line = lax.broadcasted_iota(jnp.int32, (lines, n), 0)
    picks = [line == idx[r : r + 1] for r in range(TOPK)]
    onehot = jnp.where(picks[0] | picks[1], 1.0, 0.0).astype(bf16)
    row = lax.broadcasted_iota(jnp.int32, (n, n), 0)
    col = lax.broadcasted_iota(jnp.int32, (n, n), 1)
    earlier = ((row < col) & (row // sub == col // sub)).astype(bf16)
    counts = mm(onehot, earlier)
    blk = lax.broadcasted_iota(jnp.int32, (1, n), 1) // sub
    out = []
    for r in range(TOPK):
        slot = jnp.sum(jnp.where(picks[r], counts, 0.0), axis=0, keepdims=True).astype(jnp.int32)
        out.append((idx[r : r + 1] ^ me) * (zn * capacity) + blk * capacity + slot)
    return out


def pack_body(experts, capacity, sc_ref, tok_ref, idx_ref, gain_ref, *outs):
    zn, _, sub, width = tok_ref.shape
    n = zn * sub
    x = tok_ref[...].reshape(n, width).astype(f32)
    x = (x * lax.rsqrt(jnp.mean(x * x, axis=1, keepdims=True) + epsilon) * gain_ref[...]).astype(bf16)
    t = targets(own_lanes(idx_ref[...], zn, sub, sc_ref[1]), sc_ref[0], zn, experts, capacity)
    per = zn * capacity
    line = lax.broadcasted_iota(jnp.int32, (per, n), 0)
    for m in range(experts):
        hit = (t[0] == line + m * per) | (t[1] == line + m * per)
        outs[m][...] = mm(jnp.where(hit, 1.0, 0.0).astype(bf16), x).astype(bf16)


def pack(scal, tokens, idx, gain, experts, capacity):
    zn, _, sub, width = tokens.shape
    shape = jax.ShapeDtypeStruct((zn * capacity, width), bf16)
    return pl.pallas_call(
        functools.partial(pack_body, experts, capacity),
        grid_spec=pltpu.PrefetchScalarGridSpec(
            num_scalar_prefetch=1,
            grid=(1,),
            in_specs=[
                pl.BlockSpec((zn, 1, sub, width), lambda i, s: (0, s[1], 0, 0)),
                pl.BlockSpec(idx.shape, lambda i, s: (0, 0)),
                pl.BlockSpec((1, width), lambda i, s: (0, 0)),
            ],
            out_specs=[pl.BlockSpec(shape.shape, lambda i, s: (0, 0))] * experts,
        ),
        out_shape=[shape] * experts,
        cost_estimate=pl.CostEstimate(flops=4 * 10**9, bytes_accessed=4 * 10**6, transcendentals=10**3),
        compiler_params=pltpu.CompilerParams(vmem_limit_bytes=VMEM),
        name="pack",
    )(scal, tokens, idx, gain.reshape(1, width))


def hidden_chunks(hidden):
    units, unit = (hidden // 128, 128) if hidden % 128 == 0 else (1, hidden)
    out, step = [], 1
    while units:
        take = min(step, units)
        if units - take < step:
            take = units
        out.append(take * unit)
        units -= take
        step *= 2
    return out


def ffn_body(count, pieces, chunks, *refs):
    xs = refs[:count]
    sources = refs[count : count + 6]
    outs = refs[count + 6 : count + 6 + count * len(pieces)]
    scratch = refs[count + 6 + count * len(pieces) :]
    x_ref, acc_ref, sems = scratch[0], scratch[1], scratch[2]
    buffers = scratch[3:]
    per = xs[0].shape[0]

    def copies(c):
        at = sum(chunks[:c])
        span = pl.ds(at, chunks[c])
        for k in range(3):
            for side in range(2):
                src = sources[2 * k + side].at[0]
                src = src.at[span, :] if k == 2 else src.at[:, span]
                yield pltpu.make_async_copy(src, buffers[3 * c + k].at[side], sems.at[c, 2 * k + side])

    for c in range(len(chunks)):
        for copy in copies(c):
            copy.start()
    x_ref[...] = jnp.concatenate([x[...] for x in xs], axis=0)
    for c in range(len(chunks)):
        for copy in copies(c):
            copy.wait()
        bg, bu, bd = buffers[3 * c : 3 * c + 3]
        x = x_ref[...]
        g = mm(x, jnp.concatenate([bg[0], bg[1]], axis=1))
        u = mm(x, jnp.concatenate([bu[0], bu[1]], axis=1))
        h = (g * sigmoid(g) * u).astype(bf16)
        part = mm(h, jnp.concatenate([bd[0], bd[1]], axis=0))
        if c == 0 and len(chunks) > 1:
            acc_ref[...] = part
        elif c + 1 < len(chunks):
            acc_ref[...] += part
        else:
            total = part if c == 0 else acc_ref[...] + part
            for i in range(count):
                for p, (left, right) in enumerate(pieces):
                    outs[i * len(pieces) + p][...] = total[i * per : (i + 1) * per, left:right].astype(bf16)


def ffn(xs, weights, pieces):
    count = len(xs)
    per, width = xs[0].shape
    hidden = weights[0].shape[2]
    chunks = hidden_chunks(hidden)
    buffers = []
    for c in chunks:
        buffers += [pltpu.VMEM((2, width, c), bf16), pltpu.VMEM((2, width, c), bf16), pltpu.VMEM((2, c, width), bf16)]
    whole = pl.BlockSpec((per, width), lambda: (0, 0))
    widths = [right - left for left, right in pieces]
    outs = pl.pallas_call(
        functools.partial(ffn_body, count, pieces, chunks),
        in_specs=[whole] * count + [pl.BlockSpec(memory_space=pl.ANY)] * 6,
        out_specs=[pl.BlockSpec((per, w), lambda: (0, 0)) for w in widths] * count,
        out_shape=[jax.ShapeDtypeStruct((per, w), bf16) for w in widths] * count,
        scratch_shapes=[
            pltpu.VMEM((count * per, width), bf16),
            pltpu.VMEM((count * per, width), f32),
            pltpu.SemaphoreType.DMA((len(chunks), 6)),
        ]
        + buffers,
        cost_estimate=pl.CostEstimate(flops=8 * 10**9, bytes_accessed=25 * 10**6, transcendentals=10**6),
        compiler_params=pltpu.CompilerParams(vmem_limit_bytes=FFN_VMEM),
        name="ffn",
    )(*xs, *weights)
    n = len(pieces)
    return [outs[i * n : (i + 1) * n] for i in range(count)]


def combine_body(experts, capacity, zn, lefts, cols, sc_ref, idx_ref, w_ref, *refs):
    ys = refs[:experts]
    outs = refs[experts : experts + zn]
    acc_ref = refs[-1]
    sub = outs[0].shape[0]
    n = zn * sub
    t = targets(own_lanes(idx_ref[...], zn, sub, sc_ref[1]), sc_ref[0], zn, experts, capacity)
    w = own_lanes(w_ref[...], zn, sub, sc_ref[1])
    per = zn * capacity
    line = lax.broadcasted_iota(jnp.int32, (per, n), 0)
    acc = None
    for m in range(experts):
        c = jnp.where(t[0] == line + m * per, w[0:1], 0.0)
        c = c + jnp.where(t[1] == line + m * per, w[1:2], 0.0)
        y = ys[m][:, lefts[m] : lefts[m] + cols]
        part = mm(c.astype(bf16), y, ((0,), (0,)))
        acc = part if acc is None else acc + part
    acc_ref[...] = acc.reshape(zn, sub, acc.shape[1]).astype(bf16)
    for m in range(zn):
        outs[m][...] = acc_ref[sc_ref[2] ^ m]


def combine(scal, idx, w, ys, lefts, cols, zn, sub, capacity):
    experts = len(ys)
    shape = jax.ShapeDtypeStruct((sub, cols), bf16)
    whole = lambda shape: pl.BlockSpec(shape, lambda i, s: (0, 0))
    return pl.pallas_call(
        functools.partial(combine_body, experts, capacity, zn, lefts, cols),
        grid_spec=pltpu.PrefetchScalarGridSpec(
            num_scalar_prefetch=1,
            grid=(1,),
            in_specs=[whole(idx.shape)] * 2 + [whole(y.shape) for y in ys],
            out_specs=[whole(shape.shape)] * zn,
            scratch_shapes=[pltpu.VMEM((zn, sub, cols), bf16)],
        ),
        out_shape=[shape] * zn,
        cost_estimate=pl.CostEstimate(flops=10**9, bytes_accessed=2 * 10**6, transcendentals=10**3),
        compiler_params=pltpu.CompilerParams(vmem_limit_bytes=VMEM),
        name="combine",
    )(scal, idx, w, *ys)


def columns(width, shares):
    units, out, left = width // 128, [], 0
    for p in range(len(shares)):
        right = units * sum(shares[: p + 1]) // sum(shares) * 128
        out.append((left, right))
        left = right
    return out


def on_device(
    query_preactivation,
    forget_preactivation,
    value_input_rows,
    output_gate_preactivation,
    forget_floor_gap,
    extra_log_forget,
    head_output_gain,
    mixer_output_weight,
    second_batch_tokens,
    feedforward_norm_gain,
    chosen_expert_index,
    chosen_expert_weight,
    expert_gate_weight,
    expert_up_weight,
    expert_down_weight,
):
    ep = lax.axis_size("ep")
    tp = lax.axis_size("tp")
    zn = tp // CORES
    me = lax.axis_index("ep").astype(jnp.int32)
    place = lax.axis_index("tp").astype(jnp.int32)
    zi, core = place >> 1, place & 1
    scal = jnp.stack([me, core, zi])
    over_ep = lambda x, m: lax.ppermute(x, "ep", [(i, i ^ m) for i in range(ep)])
    over_core = lambda x: lax.ppermute(x, "tp", [(i, i ^ 1) for i in range(tp)])
    over_z = lambda x, m: lax.ppermute(x, "tp", [(i, i ^ (m * CORES)) for i in range(tp)])
    tie = lax.optimization_barrier
    assert expert_gate_weight.shape[0] == 1
    experts = ep
    rows, width = second_batch_tokens.shape
    sub = rows // tp
    capacity = max(2, sub * TOPK * 5 // (4 * experts))
    cuts = columns(width, PIECES)
    pieces = len(cuts)
    extra = extra_log_forget.T
    idx = chosen_expert_index.T
    wts = chosen_expert_weight.T

    weights = []
    for w in (expert_gate_weight, expert_up_weight, expert_down_weight):
        weights += [w, over_core(w)]
    wp = over_core(mixer_output_weight)

    st = final_state(forget_preactivation, value_input_rows, forget_floor_gap, extra)
    states = [over_ep(st, m) for m in range(1, ep)]

    tokens, _ = tie((second_batch_tokens, st))
    tokens = tokens.reshape(zn, CORES, sub, width)
    packed = pack(scal, tokens, idx, feedforward_norm_gain, experts, capacity)
    order = [ep - 1] + list(range(1, ep - 1))
    arrived = {0: packed[0]}
    for m in order:
        arrived[m] = over_ep(packed[m], m)

    q, _ = tie((query_preactivation, packed[1]))
    mixed = mixer(
        scal,
        states,
        q,
        forget_preactivation,
        value_input_rows,
        output_gate_preactivation,
        forget_floor_gap,
        extra,
        head_output_gain,
    )
    gathered = [mixed]
    for m in range(1, zn):
        chained = m % 2 == 1 and m > 1
        gathered.append(over_z(gathered[m - 1] if chained else mixed, 1 if chained else m))

    x0, _ = tie((arrived[0], mixed))
    (y1,), (y0,) = ffn([arrived[ep - 1], x0], weights, [(0, width)])
    late = ffn([arrived[m] for m in order[1:]], weights, cuts)
    first_back = over_ep(y1, ep - 1)
    back = [[over_ep(late[i][p], m) for i, m in enumerate(order[1:])] for p in range(pieces)]
    own, other = project(scal, gathered, mixer_output_weight, wp)
    other = over_core(other)
    mixer_output_first = join(own, other)
    outs = []
    for p in range(pieces):
        ys = [y0] + back[p] + [first_back]
        left, right = cuts[p]
        lefts = [left] + [0] * (ep - 2) + [left]
        parts = combine(scal, idx, wts, ys, lefts, right - left, zn, sub, capacity)
        total = parts[0].astype(f32)
        for m in range(1, zn):
            total = total + over_z(parts[m], m).astype(f32)
        outs.append(total.astype(bf16))
    return mixer_output_first, jnp.concatenate(outs, axis=1)


def solution(mesh):
    placed = (
        P("ep", "tp"),
        P("ep", "tp"),
        P("ep", "tp"),
        P("ep", "tp"),
        P("tp"),
        P("ep", "tp"),
        P("tp"),
        P(None, "tp"),
        P("ep", None),
        P(),
        P("ep", None),
        P("ep", None),
        P("ep", None, "tp"),
        P("ep", None, "tp"),
        P("ep", "tp", None),
    )

    return jax.shard_map(
        on_device,
        mesh=mesh,
        in_specs=placed,
        out_specs=(P("ep", "tp"), P(("ep", "tp"), None)),
        check_vma=False,
    )
```
